32 devices in a mesh: grp: 2 (over y), dp: 2 (over x), kv: 4 (over z), tp: 2 (over core).
Axes of the slice: x: 2, y: 2, z: 4, core: 2. Of those that a mesh axis runs over, the one named last changes fastest.
Arguments:
- tokens: bfloat16 [32, 2048], P(('grp', 'dp'), ('kv', 'tp')), parts along dimension 0, may hold values from -40 to 40
- past_state: float32 [32, 16, 128, 128], P(('grp', 'dp', 'kv'), 'tp'), parts along dimension 0, may hold values from -4 to 4
- mix_gain: float32 [2048], P('kv'), may hold values from 0.1 to 1.9
- w_query: bfloat16 [2048, 2048], P('kv', 'tp'), may hold values from -0.125 to 0.125
- w_forget: bfloat16 [2048, 2048], P('kv', 'tp'), may hold values from -0.125 to 0.125
- w_value: bfloat16 [2048, 2048], P('kv', 'tp'), may hold values from -0.125 to 0.125
- w_gate_out: bfloat16 [2048, 2048], P('kv', 'tp'), may hold values from -0.125 to 0.125
- floor_logits: float32 [2048], P('tp'), may hold values from -6 to 6
- head_gain: float32 [128], replicated, may hold values from 0.1 to 1.9
- w_out: bfloat16 [2048, 2048], P(None, ('kv', 'tp')), may hold values from -0.125 to 0.125
- mlp_gain: float32 [2048], replicated, may hold values from 0.1 to 1.9
- w_gate: bfloat16 [2048, 5632], P(None, ('kv', 'tp')), may hold values from -0.125 to 0.125
- w_up: bfloat16 [2048, 5632], P(None, ('kv', 'tp')), may hold values from -0.125 to 0.125
- w_down: bfloat16 [5632, 2048], P(('kv', 'tp')), may hold values from -0.109375 to 0.109375
Outputs:
- result: bfloat16 [32, 2048], P(('grp', 'dp'), ('kv', 'tp')), parts along dimension 0
- new_state: float32 [32, 16, 128, 128], P(('grp', 'dp', 'kv'), 'tp'), parts along dimension 0
The draws below stay inside these ranges and needn't reach their ends.
There are 2 independent parts, one for each index of `grp`. The reference program is written for one: setup_inputs(seed, part) draws one part's arguments, and reference() takes and returns one part's arrays. A program takes and returns all parts, laid end to end along the dimension named above; an argument that names none is the same for every part. Nothing has to cross between parts.
All inputs are finite; a program needn't handle non-finite values.
Results may differ from the reference program's by a relative error of at most 0.0091.
Values may be sent and summed in bfloat16 or wider, within the bound.
A program may use at most 64 MiB of HBM per device.

```python
import math
import jax
import jax.numpy as jnp
from jax import lax

D = 2048
H = 16
DK = 128
DV = 128
FF = 5632
HK = 2048
HV = 2048
SEQS = 16


def draw_tokens(key, part):
    key_base = jax.random.fold_in(key, 101)
    key_rows = jax.random.fold_in(key, 202)
    columns = 10.0 ** (0.5 * (jnp.arange(D, dtype=jnp.float32) / D - 0.5))
    rows = jnp.exp(jax.random.uniform(key_rows, (SEQS, 1), jnp.float32, math.log(0.3), math.log(3.0)))
    base = jnp.clip(jax.random.normal(key_base, (SEQS, D), jnp.float32), -6.0, 6.0)
    return (base * columns * rows).astype(jnp.bfloat16)


def strengthened(drawn, key, source, target, blocks, factor):
    def block_of(position):
        return (jnp.arange(drawn.shape[position]) // (drawn.shape[position] // blocks)).reshape((-1,) + (1,) * (drawn.ndim - 1 - position))

    first = jax.random.permutation(key, blocks)[block_of(target)]
    far = (block_of(target) + blocks // 2) % blocks
    return jnp.where((block_of(source) == first) | (block_of(source) == far), factor * drawn, drawn)


def block_levels(stream_key, shape, split, least, largest):
    factor_of, own = 1.0, jax.random.fold_in(stream_key, 6)
    for position, parts in split:
        draws = jnp.exp(jax.random.uniform(jax.random.fold_in(own, position), (parts,), jnp.float32, least / len(split), largest / len(split)))
        factor_of = factor_of * jnp.repeat(draws, shape[position] // parts).reshape([-1 if axis == position else 1 for axis in range(len(shape))])
    return factor_of


def bell_draw(own_key, extent, deviation, limit, pieces=(), kind=jnp.bfloat16):
    values = jax.random.normal(own_key, extent, jnp.float32) * deviation
    if len(pieces) > 0:
        values = block_levels(own_key, extent, pieces, -0.22, 0.18) * values
    return jnp.clip(values, min=-limit, max=limit).astype(kind)


def bell_draw_with(rng, shape, spread, bound, shards, heavy, held_as=jnp.bfloat16):
    array = spread * jax.random.normal(rng, shape, jnp.float32)
    if shards:
        array = array * block_levels(rng, shape, shards, -0.22, 0.18)
    return jnp.clip(strengthened(array, jax.random.fold_in(rng, 3), *heavy), -bound, bound).astype(held_as)


def setup_inputs(seed: int = 0, part: int = 0) -> dict:
    keys = jax.random.split(jax.random.key(seed), 15)
    own_keys = jax.random.split(jax.random.fold_in(keys[14], part), 15)
    tokens = draw_tokens(jax.random.fold_in(jax.random.fold_in(keys[14], part), 71), part)
    past_state = bell_draw(own_keys[1], (SEQS, H, DK, DV), 0.5, 4.0, ((0, 8), (1, 2)), jnp.float32)
    mix_gain = jnp.clip(1.0 + 0.18 * jax.random.normal(keys[2], (D,), jnp.float32), 0.1, 1.9)
    w_query = bell_draw(keys[3], (D, HK), D ** -0.5, 0.125, ((0, 4), (1, 2)))
    w_forget = bell_draw(keys[4], (D, HK), D ** -0.5, 0.125, ((0, 4), (1, 2)))
    w_value = bell_draw(keys[5], (D, HV), D ** -0.5, 0.125, ((0, 4), (1, 2)))
    w_gate_out = bell_draw(keys[6], (D, HV), D ** -0.5, 0.125, ((0, 4), (1, 2)))
    floor_logits = bell_draw(keys[7], (HK,), 1.5, 6.0, ((0, 2),), jnp.float32)
    head_gain = jnp.clip(1.0 + 0.18 * jax.random.normal(keys[8], (DV,), jnp.float32), 0.1, 1.9)
    w_out = bell_draw(keys[9], (HV, D), HV ** -0.5, 0.125, ((1, 8),))
    mlp_gain = jnp.clip(1.0 + 0.18 * jax.random.normal(keys[10], (D,), jnp.float32), 0.1, 1.9)
    w_gate = bell_draw(keys[11], (D, FF), D ** -0.5, 0.125, ((1, 8),))
    w_up = bell_draw(keys[12], (D, FF), D ** -0.5, 0.125, ((1, 8),))
    w_down = bell_draw_with(keys[13], (FF, D), FF ** -0.5, 0.109375, ((0, 8),), (0, 1, 8, 2.0))
    return dict(tokens=tokens, past_state=past_state, mix_gain=mix_gain, w_query=w_query, w_forget=w_forget, w_value=w_value, w_gate_out=w_gate_out, floor_logits=floor_logits, head_gain=head_gain, w_out=w_out, mlp_gain=mlp_gain, w_gate=w_gate, w_up=w_up, w_down=w_down)


epsilon = 1e-06

def reference(tokens, past_state, mix_gain, w_query, w_forget, w_value, w_gate_out, floor_logits, head_gain, w_out, mlp_gain, w_gate, w_up, w_down):
    count = tokens.shape[0]
    token_f = tokens.astype(jnp.float32)
    row_scale = lax.rsqrt(lax.optimization_barrier(jnp.mean(token_f * token_f, axis=1, keepdims=True)) + epsilon)
    gained = (token_f * mix_gain).astype(jnp.bfloat16)
    query = jnp.dot(gained, w_query, preferred_element_type=jnp.float32) * row_scale
    forget_pre = jnp.dot(gained, w_forget, preferred_element_type=jnp.float32) * row_scale
    value = jnp.dot(gained, w_value, preferred_element_type=jnp.float32) * row_scale
    gate_pre = jnp.dot(gained, w_gate_out, preferred_element_type=jnp.float32) * row_scale
    lower = jax.nn.sigmoid(floor_logits).reshape(H, DK)
    forget = lower + (1.0 - lower) * jax.nn.sigmoid(forget_pre.reshape(count, H, DK))
    values = value.reshape(count, H, DV)
    new_state = forget[..., None] * past_state + (1.0 - forget)[..., None] * values[:, :, None, :]
    activ = jax.nn.silu(query.reshape(count, H, DK))
    head_out = jnp.einsum('shkv,shk->shv', new_state, activ, precision=lax.Precision.HIGHEST)
    normed = head_out * lax.rsqrt(lax.optimization_barrier(jnp.mean(head_out * head_out, axis=2, keepdims=True)) + epsilon)
    normed = normed * head_gain * jax.nn.silu(gate_pre.reshape(count, H, DV))
    mixed = normed.reshape(count, H * DV).astype(jnp.bfloat16)
    middle = (token_f + jnp.dot(mixed, w_out, preferred_element_type=jnp.float32)).astype(jnp.bfloat16)
    middle_f = middle.astype(jnp.float32)
    mlp_scale = lax.rsqrt(lax.optimization_barrier(jnp.mean(middle_f * middle_f, axis=1, keepdims=True)) + epsilon)
    mlp_in = (middle_f * mlp_scale * mlp_gain).astype(jnp.bfloat16)
    gate = jnp.dot(mlp_in, w_gate, preferred_element_type=jnp.float32)
    upward = jnp.dot(mlp_in, w_up, preferred_element_type=jnp.float32)
    hidden = (jax.nn.silu(gate) * upward).astype(jnp.bfloat16)
    result = (middle_f + jnp.dot(hidden, w_down, preferred_element_type=jnp.float32)).astype(jnp.bfloat16)
    return (result, new_state)
```

```python
import functools

import jax
import jax.numpy as jnp
from jax import lax
from jax.experimental import pallas as pl
from jax.experimental.pallas import tpu as pltpu
from jax.sharding import PartitionSpec as P

epsilon = 1e-06
F32 = jnp.float32
BF16 = jnp.bfloat16
MESH = pl.DeviceIdType.MESH


def sigmoid(a):
    return 1.0 / (1.0 + jnp.exp(-a))


def silu(a):
    return a / (1.0 + jnp.exp(-a))


def dot_t(a, b):
    return lax.dot_general(a, b, (((1,), (1,)), ((), ())), preferred_element_type=F32)


def kernel(
    K,
    T,
    tokens,
    past,
    mix_gain,
    w_query,
    w_forget,
    w_value,
    w_gate_out,
    floor_logits,
    head_gain,
    w_out,
    mlp_gain,
    w_gate,
    w_up,
    w_down,
    result,
    new_state,
    tok_v,
    past_v,
    mixg_v,
    proj_v,
    floor_v,
    hgain_v,
    wout_v,
    mlpg_v,
    wgate_v,
    wup_v,
    wdown_v,
    sq_send,
    sq_recv,
    part,
    part_send,
    part_recv,
    split_v,
    mix_all,
    mix_f,
    mid_all,
    term_send,
    term_recv,
    local_sem,
    tok_ss,
    tok_rs,
    sq_ss,
    sq_rs,
    part_ss,
    part_rs,
    mix_ss,
    mix_rs,
    mid_ss,
    mid_rs,
    term_ss,
    term_rs,
):
    R, W = tokens.shape
    RL, H, DK, DV = past.shape
    D = w_gate.shape[1]
    kv = lax.axis_index("kv")
    tp = lax.axis_index("tp")
    me = kv * T + tp

    paired = K & (K - 1) == 0
    hops = list(range(1, K))
    near = [(0, dt) for dt in range(1, T)] + [(dk, dt) for dk in hops for dt in range(T)]

    def flip(k, dk):
        bit = 1
        while bit <= dk:
            if dk & bit:
                k = k + bit - 2 * bit * lax.rem(k // bit, 2)
            bit *= 2
        return k

    def other(dk, dt):
        k = flip(kv, dk) if paired else lax.rem(kv + dk, K)
        return k, (lax.rem(tp + dt, T) if dk == 0 else dt)

    def source(dk, dt):
        k = flip(kv, dk) if paired else lax.rem(kv + K - dk, K)
        return k, (lax.rem(tp + T - dt, T) if dk == 0 else T - 1 - dt)

    def load(i, src, dst):
        copy = pltpu.make_async_copy(src, dst, local_sem.at[i])
        copy.start()
        return copy

    c_tok = load(0, tokens, tok_v.at[tp])
    c_mixg = load(1, mix_gain, mixg_v)
    c_proj = [
        load(2 + i, w, proj_v.at[i])
        for i, w in enumerate((w_forget, w_query, w_value, w_gate_out))
    ]
    c_past = load(6, past, past_v)
    c_floor = load(7, floor_logits, floor_v)
    c_hgain = load(8, head_gain, hgain_v)
    c_mlpg = load(9, mlp_gain, mlpg_v)
    c_wout = load(10, w_out, wout_v)
    c_wgate = load(11, w_gate, wgate_v)
    c_wup = load(12, w_up, wup_v)
    c_wdown = load(13, w_down, wdown_v)

    barrier = pltpu.get_barrier_semaphore()
    for dk, dt in near:
        k, t = other(dk, dt)
        pl.semaphore_signal(barrier, inc=1, device_id={"kv": k, "tp": t}, device_id_type=MESH)
    c_tok.wait()
    pl.semaphore_wait(barrier, len(near))

    def send(src, dst, ss, rs, k, t):
        copy = pltpu.make_async_remote_copy(
            src_ref=src,
            dst_ref=dst,
            send_sem=ss,
            recv_sem=rs,
            device_id={"kv": k, "tp": t},
            device_id_type=MESH,
        )
        copy.start()
        return copy

    def arrived(dst, ss, rs):
        pltpu.make_async_remote_copy(
            src_ref=dst,
            dst_ref=dst,
            send_sem=ss,
            recv_sem=rs,
            device_id={"kv": kv, "tp": lax.rem(tp + 1, T)},
            device_id_type=MESH,
        ).wait_recv()

    sent = []
    for dt in range(1, T):
        k, t = other(0, dt)
        sent.append(send(tok_v.at[tp], tok_v.at[tp], tok_ss.at[dt], tok_rs.at[tp], k, t))

    c_mixg.wait()
    gained = []
    early = []
    square = jnp.zeros((R, 1), F32)
    for dt in range(T):
        t = lax.rem(tp + T - dt, T)
        if dt:
            arrived(tok_v.at[t], tok_ss.at[0], tok_rs.at[t])
        block = tok_v[t].astype(F32)
        square = square + jnp.sum(block * block, axis=1, keepdims=True)
        gained.append((block * mixg_v[t]).astype(BF16))
        if dt == 0:
            rows = pl.ds(pl.multiple_of(t * W, W), W)
            for i in range(4):
                c_proj[i].wait()
                early.append(
                    jnp.dot(gained[0], proj_v[i, rows, :], preferred_element_type=F32)
                )
    square = jnp.broadcast_to(square, (R, DK))
    for k in range(K):
        sq_send[k] = square[k * RL : (k + 1) * RL]
    for dk in hops[::-1]:
        k, t = other(dk, 0)[0], tp
        sent.append(
            send(sq_send.at[k], sq_recv.at[kv], sq_ss.at[dk], sq_rs.at[kv], k, t)
        )
    for i in range(4):
        total = early[i]
        for dt in range(1, T):
            t = lax.rem(tp + T - dt, T)
            rows = pl.ds(pl.multiple_of(t * W, W), W)
            piece = jnp.dot(gained[dt], proj_v[i, rows, :], preferred_element_type=F32)
            total = total + piece
        for h in range(H):
            part[i, :, h, :] = total[:, h * DK : (h + 1) * DK]
        for k in range(K):
            part_send[i, k] = part[i, k * RL : (k + 1) * RL].reshape(RL * H, DK).astype(BF16)
        for dk in hops[::-1]:
            k, t = other(dk, 0)[0], tp
            sent.append(
                send(
                    part_send.at[i, k],
                    part_recv.at[i, kv],
                    part_ss.at[i, dk],
                    part_rs.at[i, kv],
                    k,
                    t,
                )
            )

    c_floor.wait()
    c_hgain.wait()
    lower = sigmoid(floor_v[...])
    lower = jnp.concatenate([lower] * RL, axis=0)
    c_past.wait()
    for s in range(RL):
        for h in range(H):
            rows = pl.ds((s * H + h) * DK, DK)
            block = past_v[s, h]
            high = block.astype(BF16)
            split_v[rows, :DV] = high
            split_v[rows, DV:] = (block - high.astype(F32)).astype(BF16)
    square = sq_send[kv]
    for dk in hops:
        k, t = source(dk, 0)
        arrived(sq_recv.at[k], sq_ss.at[dk], sq_rs.at[k])
        square = square + sq_recv[k]
    row_scale = lax.rsqrt(square / D + epsilon)
    row_scale = jnp.concatenate(
        [jnp.broadcast_to(row_scale[s : s + 1], (H, DK)) for s in range(RL)], axis=0
    )

    def summed(i):
        total = part[i, pl.ds(kv * RL, RL)].reshape(RL * H, DK)
        for dk in hops:
            k, t = source(dk, 0)
            arrived(part_recv.at[i, k], part_ss.at[i, dk], part_rs.at[i, k])
            total = total + part_recv[i, k].astype(F32)
        return total * row_scale

    forget = lower + (1.0 - lower) * sigmoid(summed(0))
    activ = silu(summed(1))
    weight = activ * forget
    high = weight.astype(BF16).astype(F32)
    weight = jnp.concatenate([high, weight - high], axis=0)
    owner = lax.rem(lax.broadcasted_iota(jnp.int32, weight.shape, 0), RL * H)
    left = jnp.concatenate(
        [jnp.where(owner == i, weight, 0.0).astype(BF16) for i in range(RL * H)], axis=1
    )
    wide = jnp.dot(left, split_v[...], preferred_element_type=F32)
    head_out = wide[: RL * H, :DV] + (wide[: RL * H, DV:] + wide[RL * H :, :DV])
    rest = jnp.sum(activ * (1.0 - forget), axis=1, keepdims=True)
    value = summed(2)
    head_out = head_out + value * rest
    normed = head_out * lax.rsqrt(
        jnp.mean(head_out * head_out, axis=1, keepdims=True) + epsilon
    )
    mixed = normed * hgain_v[...] * silu(summed(3))
    mix_all[tp, kv] = mixed.astype(BF16)
    for dk, dt in near[::-1]:
        k, t = other(dk, dt)
        slot = mix_all.at[tp, kv]
        sent.append(send(slot, slot, mix_ss.at[dk, dt], mix_rs.at[kv, tp], k, t))

    columns = forget.T
    for s in range(RL):
        for h in range(H):
            i = s * H + h
            row = value[i : i + 1, :]
            new_state[s, h] = row + columns[:, i : i + 1] * (past_v[s, h] - row)

    def spread(t, k):
        mix_f[t, pl.ds(k * RL, RL)] = mix_all[t, k].astype(F32).reshape(RL, H, DV)

    spread(tp, kv)
    for dk, dt in near:
        k, t = source(dk, dt)
        arrived(mix_all.at[t, k], mix_ss.at[dk, dt], mix_rs.at[k, t])
        spread(t, k)
    every_head = jnp.concatenate(
        [mix_f[t, :, h, :].astype(BF16) for t in range(T) for h in range(H)], axis=1
    )
    c_wout.wait()
    middle = tok_v[tp].astype(F32) + jnp.dot(
        every_head, wout_v[...], preferred_element_type=F32
    )
    middle = middle.astype(BF16)
    mid_all[me] = middle
    for dk, dt in near[::-1]:
        k, t = other(dk, dt)
        slot = mid_all.at[me]
        sent.append(send(slot, slot, mid_ss.at[dk, dt], mid_rs.at[kv, tp], k, t))

    c_mlpg.wait()
    square = jnp.zeros((R, 1), F32)
    gate = None
    if W % 128 == 0:
        groups = [[peer] for peer in [(0, 0)] + near]
    else:
        groups = [[(dk, dt) for dt in range(T)] for dk in [0] + hops]
    for group in groups:
        for dk, dt in group:
            k, t = source(dk, dt)
            if dk or dt:
                arrived(mid_all.at[k * T + t], mid_ss.at[dk, dt], mid_rs.at[k, t])
        k, t = source(*group[0])
        j = k * T + (t if len(group) == 1 else 0)
        blocks = []
        for i in range(len(group)):
            block = mid_all[j + i].astype(F32)
            square = square + jnp.sum(block * block, axis=1, keepdims=True)
            blocks.append((block * mlpg_v[j + i]).astype(BF16))
        block = jnp.concatenate(blocks, axis=1) if len(blocks) > 1 else blocks[0]
        width = len(group) * W
        lanes = pl.ds(pl.multiple_of(j * W, width), width)
        if gate is None:
            c_wgate.wait()
        g = dot_t(block, wgate_v[:, lanes])
        if gate is None:
            c_wup.wait()
        u = dot_t(block, wup_v[:, lanes])
        gate, upward = (g, u) if gate is None else (gate + g, upward + u)
    mlp_scale = lax.rsqrt(square / D + epsilon)
    hidden = (silu(gate * mlp_scale) * (upward * mlp_scale)).astype(BF16)
    c_wdown.wait()
    for dk in hops[::-1] + [0]:
        k, _ = other(dk, 0)
        lanes = pl.ds(pl.multiple_of(k * T * W, T * W), T * W)
        chunk = jnp.dot(hidden, wdown_v[:, lanes], preferred_element_type=F32).astype(BF16)
        for t in range(T):
            term_send[k * T + t] = chunk[:, t * W : (t + 1) * W]
        for dt in range(0 if dk else 1, T):
            _, t = other(dk, dt)
            sent.append(
                send(
                    term_send.at[k * T + t],
                    term_recv.at[me],
                    term_ss.at[dk, dt],
                    term_rs.at[kv, tp],
                    k,
                    t,
                )
            )
    total = term_send[me].astype(F32)
    for dk, dt in near:
        k, t = source(dk, dt)
        j = k * T + t
        arrived(term_recv.at[j], term_ss.at[dk, dt], term_rs.at[k, t])
        total = total + term_recv[j].astype(F32)
    result[...] = (middle.astype(F32) + total).astype(BF16)
    for copy in sent:
        copy.wait_send()


def body(
    tokens,
    past_state,
    mix_gain,
    w_query,
    w_forget,
    w_value,
    w_gate_out,
    floor_logits,
    head_gain,
    w_out,
    mlp_gain,
    w_gate,
    w_up,
    w_down,
):
    K = lax.axis_size("kv")
    T = lax.axis_size("tp")
    n = K * T
    R, W = tokens.shape
    RL, H, DK, DV = past_state.shape
    args = (
        tokens,
        past_state,
        mix_gain.reshape(T, 1, W),
        w_query,
        w_forget,
        w_value,
        w_gate_out,
        floor_logits.reshape(H, DK),
        head_gain.reshape(1, DV),
        w_out,
        mlp_gain.reshape(n, 1, W),
        w_gate.T,
        w_up.T,
        w_down,
    )
    V = pltpu.VMEM
    dma = pltpu.SemaphoreType.DMA
    anywhere = pl.BlockSpec(memory_space=pl.ANY)
    return pl.pallas_call(
        functools.partial(kernel, K, T),
        out_shape=(
            pltpu.VMEM((R, W), BF16),
            pltpu.VMEM(past_state.shape, F32),
        ),
        in_specs=[anywhere] * len(args),
        out_specs=(pl.BlockSpec(memory_space=pltpu.VMEM),)*2,
        scratch_shapes=[
            V((T, R, W), BF16),
            V(past_state.shape, F32),
            V((T, 1, W), F32),
            V((4,) + w_query.shape, BF16),
            V((H, DK), F32),
            V((1, DV), F32),
            V(w_out.shape, BF16),
            V((n, 1, W), F32),
            V(w_gate.shape[::-1], BF16),
            V(w_up.shape[::-1], BF16),
            V(w_down.shape, BF16),
            V((K, RL, DK), F32),
            V((K, RL, DK), F32),
            V((4, R, H, DK), F32),
            V((4, K, RL * H, DK), BF16),
            V((4, K, RL * H, DK), BF16),
            V((RL * H * DK, 2 * DV), BF16),
            V((T, K, RL * H, DV), BF16),
            V((T, R, H, DV), F32),
            V((n, R, W), BF16),
            V((n, R, W), BF16),
            V((n, R, W), BF16),
            dma((14,)),
            dma((T,)),
            dma((T,)),
            dma((K,)),
            dma((K,)),
            dma((4, K)),
            dma((4, K)),
            dma((K, T)),
            dma((K, T)),
            dma((K, T)),
            dma((K, T)),
            dma((K, T)),
            dma((K, T)),
        ],
        compiler_params=pltpu.CompilerParams(
            collective_id=0, has_side_effects=True, vmem_limit_bytes=60 * 1024 * 1024
        ),
    )(*args)


def solution(mesh):
    placed = (
        P(("grp", "dp"), ("kv", "tp")),
        P(("grp", "dp", "kv"), "tp", None, None),
        P("kv"),
        P("kv", "tp"),
        P("kv", "tp"),
        P("kv", "tp"),
        P("kv", "tp"),
        P("tp"),
        P(),
        P(None, ("kv", "tp")),
        P(),
        P(None, ("kv", "tp")),
        P(None, ("kv", "tp")),
        P(("kv", "tp"), None),
    )
    return jax.shard_map(
        body,
        mesh=mesh,
        in_specs=placed,
        out_specs=(P(("grp", "dp"), ("kv", "tp")), P(("grp", "dp", "kv"), "tp", None, None)),
        check_vma=False,
    )
```

```python
import functools

import jax
import jax.numpy as jnp
from jax import lax
from jax.experimental import pallas as pl
from jax.experimental.pallas import tpu as pltpu
from jax.sharding import PartitionSpec as P

epsilon = 1e-06
F32 = jnp.float32
BF16 = jnp.bfloat16
MESH = pl.DeviceIdType.MESH


def sigmoid(a):
    return 1.0 / (1.0 + jnp.exp(-a))


def silu(a):
    return a / (1.0 + jnp.exp(-a))


def dot_t(a, b):
    return lax.dot_general(a, b, (((1,), (1,)), ((), ())), preferred_element_type=F32)


def kernel(
    K,
    T,
    tokens,
    past,
    mix_gain,
    w_query,
    w_forget,
    w_value,
    w_gate_out,
    floor_logits,
    head_gain,
    w_out,
    mlp_gain,
    w_gate,
    w_up,
    w_down,
    result,
    new_state,
    tok_v,
    past_v,
    mixg_v,
    proj_v,
    floor_v,
    hgain_v,
    wout_v,
    mlpg_v,
    wgate_v,
    wup_v,
    wdown_v,
    sq_send,
    sq_recv,
    part,
    part_send,
    part_recv,
    split_v,
    mix_all,
    mix_f,
    mid_all,
    term_send,
    term_recv,
    local_sem,
    tok_ss,
    tok_rs,
    sq_ss,
    sq_rs,
    part_ss,
    part_rs,
    mix_ss,
    mix_rs,
    mid_ss,
    mid_rs,
    term_ss,
    term_rs,
):
    R, W = tokens.shape
    RL, H, DK, DV = past.shape
    D = w_gate.shape[1]
    kv = lax.axis_index("kv")
    tp = lax.axis_index("tp")
    me = kv * T + tp

    hops = list(range(1, K))
    near = [(0, dt) for dt in range(1, T)] + [(j, dt) for j in hops for dt in range(T)]
    upper = (2 * kv) // K
    short = upper * (K - 1 - kv) + (1 - upper) * kv
    ahead = 1 - 2 * upper

    def hop(j):
        if j == 0:
            return kv
        both = jnp.minimum(jnp.maximum(2 * short - j + 1, 0), 1)
        step = both * ((j + 1) // 2) * (2 * (j % 2) - 1) + (1 - both) * (j - short)
        return kv + ahead * step

    def other(j, dt):
        return hop(j), (lax.rem(tp + dt, T) if j == 0 else dt)

    def source(j, dt):
        return hop(j), (lax.rem(tp + T - dt, T) if j == 0 else T - 1 - dt)

    def load(i, src, dst):
        copy = pltpu.make_async_copy(src, dst, local_sem.at[i])
        copy.start()
        return copy

    c_tok = load(0, tokens, tok_v.at[tp])
    c_mixg = load(1, mix_gain, mixg_v)
    c_proj = [
        load(2 + i, w, proj_v.at[i])
        for i, w in enumerate((w_forget, w_query, w_value, w_gate_out))
    ]
    c_past = load(6, past, past_v)
    c_floor = load(7, floor_logits, floor_v)
    c_hgain = load(8, head_gain, hgain_v)
    c_mlpg = load(9, mlp_gain, mlpg_v)

    barrier = pltpu.get_barrier_semaphore()

    def signal(k, t):
        pl.semaphore_signal(barrier, inc=1, device_id={"kv": k, "tp": t}, device_id_type=MESH)

    for j in hops[::-1]:
        signal(hop(j), 0)
    signal(kv, 1 - tp)
    c_tok.wait()

    def send(src, dst, ss, rs, k, t):
        copy = pltpu.make_async_remote_copy(
            src_ref=src,
            dst_ref=dst,
            send_sem=ss,
            recv_sem=rs,
            device_id={"kv": k, "tp": t},
            device_id_type=MESH,
        )
        copy.start()
        return copy

    def arrived(dst, ss, rs):
        pltpu.make_async_remote_copy(
            src_ref=dst,
            dst_ref=dst,
            send_sem=ss,
            recv_sem=rs,
            device_id={"kv": kv, "tp": lax.rem(tp + 1, T)},
            device_id_type=MESH,
        ).wait_recv()

    sent = []
    swap = pltpu.make_async_remote_copy(
        src_ref=tok_v.at[tp],
        dst_ref=tok_v.at[tp],
        send_sem=tok_ss,
        recv_sem=tok_rs,
        device_id={"kv": kv, "tp": 1 - tp},
        device_id_type=MESH,
    )
    sent.append(swap)

    @pl.when(tp == 1)
    def _():
        pl.semaphore_wait(barrier, 1)
        swap.start()

    c_mixg.wait()

    def features(t):
        block = tok_v[t].astype(F32)
        square = jnp.sum(block * block, axis=1, keepdims=True)
        rows = pl.ds(pl.multiple_of(t * W, W), W)
        return (block * mixg_v[t]).astype(BF16), rows, square

    def project(part_of, i):
        gained, rows, _ = part_of
        return jnp.dot(gained, proj_v[i, rows, :], preferred_element_type=F32)

    def spread_out(i, total):
        for h in range(H):
            part[i, :, h, :] = total[:, h * DK : (h + 1) * DK]
        for k in range(K):
            part_send[i, k] = part[i, k * RL : (k + 1) * RL].reshape(RL * H, DK).astype(BF16)

    def scatter(i):
        for j in hops[::-1]:
            k = hop(j)
            sent.append(
                send(
                    part_send.at[i, k],
                    part_recv.at[i, kv],
                    part_ss.at[i, j],
                    part_rs.at[i, kv],
                    k,
                    tp,
                )
            )

    mine = features(tp)
    early = []
    for i in range(2):
        c_proj[i].wait()
        early.append(project(mine, i))
    swap.wait_recv()
    theirs = features(1 - tp)
    square = jnp.broadcast_to(mine[2] + theirs[2], (R, DK))
    for k in range(K):
        sq_send[k] = square[k * RL : (k + 1) * RL]
    totals = [early[i] + project(theirs, i) for i in range(2)]
    spread_out(0, totals[0])
    spread_out(1, totals[1])

    @pl.when(tp == 0)
    def _():
        pl.semaphore_wait(barrier, K * T - 1)
        swap.start()

    for j in hops[::-1]:
        k = hop(j)
        sent.append(send(sq_send.at[k], sq_recv.at[kv], sq_ss.at[j], sq_rs.at[kv], k, tp))
    scatter(0)
    scatter(1)
    c_wout = load(10, w_out, wout_v)
    c_wgate = load(11, w_gate, wgate_v)
    c_wup = load(12, w_up, wup_v)
    c_wdown = load(13, w_down, wdown_v)
    totals = []
    for i in range(2, 4):
        c_proj[i].wait()
        totals.append(project(mine, i) + project(theirs, i))
    for i in range(2, 4):
        spread_out(i, totals[i - 2])
        scatter(i)

    c_floor.wait()
    c_hgain.wait()
    lower = sigmoid(floor_v[...])
    lower = jnp.concatenate([lower] * RL, axis=0)
    c_past.wait()
    for s in range(RL):
        for h in range(H):
            rows = pl.ds((s * H + h) * DK, DK)
            block = past_v[s, h]
            high = block.astype(BF16)
            split_v[rows, :DV] = high
            split_v[rows, DV:] = (block - high.astype(F32)).astype(BF16)
    square = sq_send[kv]
    for dk in hops:
        k, t = source(dk, 0)
        arrived(sq_recv.at[k], sq_ss.at[dk], sq_rs.at[k])
        square = square + sq_recv[k]
    row_scale = lax.rsqrt(square / D + epsilon)
    row_scale = jnp.concatenate(
        [jnp.broadcast_to(row_scale[s : s + 1], (H, DK)) for s in range(RL)], axis=0
    )

    def summed(i):
        total = part[i, pl.ds(kv * RL, RL)].reshape(RL * H, DK)
        for dk in hops:
            k, t = source(dk, 0)
            arrived(part_recv.at[i, k], part_ss.at[i, dk], part_rs.at[i, k])
            total = total + part_recv[i, k].astype(F32)
        return total * row_scale

    forget = lower + (1.0 - lower) * sigmoid(summed(0))
    activ = silu(summed(1))
    weight = activ * forget
    high = weight.astype(BF16).astype(F32)
    weight = jnp.concatenate([high, weight - high], axis=0)
    owner = lax.rem(lax.broadcasted_iota(jnp.int32, weight.shape, 0), RL * H)
    left = jnp.concatenate(
        [jnp.where(owner == i, weight, 0.0).astype(BF16) for i in range(RL * H)], axis=1
    )
    wide = jnp.dot(left, split_v[...], preferred_element_type=F32)
    head_out = wide[: RL * H, :DV] + (wide[: RL * H, DV:] + wide[RL * H :, :DV])
    rest = jnp.sum(activ * (1.0 - forget), axis=1, keepdims=True)
    value = summed(2)
    head_out = head_out + value * rest
    normed = head_out * lax.rsqrt(
        jnp.mean(head_out * head_out, axis=1, keepdims=True) + epsilon
    )
    mixed = normed * hgain_v[...] * silu(summed(3))
    mix_all[tp, kv] = mixed.astype(BF16)
    for dk, dt in near[::-1]:
        k, t = other(dk, dt)
        slot = mix_all.at[tp, kv]
        sent.append(send(slot, slot, mix_ss.at[dk, dt], mix_rs.at[kv, tp], k, t))

    columns = forget.T
    for s in range(RL):
        for h in range(H):
            i = s * H + h
            row = value[i : i + 1, :]
            new_state[s, h] = row + columns[:, i : i + 1] * (past_v[s, h] - row)

    def spread(t, k):
        mix_f[t, pl.ds(k * RL, RL)] = mix_all[t, k].astype(F32).reshape(RL, H, DV)

    spread(tp, kv)
    for dk, dt in near:
        k, t = source(dk, dt)
        arrived(mix_all.at[t, k], mix_ss.at[dk, dt], mix_rs.at[k, t])
        spread(t, k)
    every_head = jnp.concatenate(
        [mix_f[t, :, h, :].astype(BF16) for t in range(T) for h in range(H)], axis=1
    )
    c_wout.wait()
    middle = tok_v[tp].astype(F32) + jnp.dot(
        every_head, wout_v[...], preferred_element_type=F32
    )
    middle = middle.astype(BF16)
    mid_all[me] = middle
    for dk, dt in near[::-1]:
        k, t = other(dk, dt)
        slot = mid_all.at[me]
        sent.append(send(slot, slot, mid_ss.at[dk, dt], mid_rs.at[kv, tp], k, t))

    c_mlpg.wait()
    square = jnp.zeros((R, 1), F32)
    gate = None
    if W % 128 == 0:
        groups = [[peer] for peer in [(0, 0)] + near]
    else:
        groups = [[(dk, dt) for dt in range(T)] for dk in [0] + hops]
    for group in groups:
        for dk, dt in group:
            k, t = source(dk, dt)
            if dk or dt:
                arrived(mid_all.at[k * T + t], mid_ss.at[dk, dt], mid_rs.at[k, t])
        k, t = source(*group[0])
        j = k * T + (t if len(group) == 1 else 0)
        blocks = []
        for i in range(len(group)):
            block = mid_all[j + i].astype(F32)
            square = square + jnp.sum(block * block, axis=1, keepdims=True)
            blocks.append((block * mlpg_v[j + i]).astype(BF16))
        block = jnp.concatenate(blocks, axis=1) if len(blocks) > 1 else blocks[0]
        width = len(group) * W
        lanes = pl.ds(pl.multiple_of(j * W, width), width)
        if gate is None:
            c_wgate.wait()
        g = dot_t(block, wgate_v[:, lanes])
        if gate is None:
            c_wup.wait()
        u = dot_t(block, wup_v[:, lanes])
        gate, upward = (g, u) if gate is None else (gate + g, upward + u)
    mlp_scale = lax.rsqrt(square / D + epsilon)
    hidden = (silu(gate * mlp_scale) * (upward * mlp_scale)).astype(BF16)
    c_wdown.wait()
    for dk in hops[::-1] + [0]:
        k, _ = other(dk, 0)
        lanes = pl.ds(pl.multiple_of(k * T * W, T * W), T * W)
        chunk = jnp.dot(hidden, wdown_v[:, lanes], preferred_element_type=F32).astype(BF16)
        for t in range(T):
            term_send[k * T + t] = chunk[:, t * W : (t + 1) * W]
        for dt in range(0 if dk else 1, T):
            _, t = other(dk, dt)
            sent.append(
                send(
                    term_send.at[k * T + t],
                    term_recv.at[me],
                    term_ss.at[dk, dt],
                    term_rs.at[kv, tp],
                    k,
                    t,
                )
            )
    total = term_send[me].astype(F32)
    for dk, dt in near:
        k, t = source(dk, dt)
        j = k * T + t
        arrived(term_recv.at[j], term_ss.at[dk, dt], term_rs.at[k, t])
        total = total + term_recv[j].astype(F32)
    result[...] = (middle.astype(F32) + total).astype(BF16)
    for copy in sent:
        copy.wait_send()


def flush(result_v, state_v, result, new_state, sem):
    copies = [
        pltpu.make_async_copy(state_v, new_state, sem.at[0]),
        pltpu.make_async_copy(result_v, result, sem.at[1]),
    ]
    for copy in copies:
        copy.start()
    for copy in copies:
        copy.wait()


def body(
    tokens,
    past_state,
    mix_gain,
    w_query,
    w_forget,
    w_value,
    w_gate_out,
    floor_logits,
    head_gain,
    w_out,
    mlp_gain,
    w_gate,
    w_up,
    w_down,
):
    K = lax.axis_size("kv")
    T = lax.axis_size("tp")
    assert T == 2
    n = K * T
    R, W = tokens.shape
    RL, H, DK, DV = past_state.shape
    args = (
        tokens,
        past_state,
        mix_gain.reshape(T, 1, W),
        w_query,
        w_forget,
        w_value,
        w_gate_out,
        floor_logits.reshape(H, DK),
        head_gain.reshape(1, DV),
        w_out,
        mlp_gain.reshape(n, 1, W),
        w_gate.T,
        w_up.T,
        w_down,
    )
    V = pltpu.VMEM
    dma = pltpu.SemaphoreType.DMA
    anywhere = pl.BlockSpec(memory_space=pl.ANY)
    outs = pl.pallas_call(
        functools.partial(kernel, K, T),
        out_shape=(
            pltpu.VMEM((R, W), BF16),
            pltpu.VMEM(past_state.shape, F32),
        ),
        in_specs=[anywhere] * len(args),
        out_specs=(pl.BlockSpec(memory_space=pltpu.VMEM),)*2,
        scratch_shapes=[
            V((T, R, W), BF16),
            V(past_state.shape, F32),
            V((T, 1, W), F32),
            V((4,) + w_query.shape, BF16),
            V((H, DK), F32),
            V((1, DV), F32),
            V(w_out.shape, BF16),
            V((n, 1, W), F32),
            V(w_gate.shape[::-1], BF16),
            V(w_up.shape[::-1], BF16),
            V(w_down.shape, BF16),
            V((K, RL, DK), F32),
            V((K, RL, DK), F32),
            V((4, R, H, DK), F32),
            V((4, K, RL * H, DK), BF16),
            V((4, K, RL * H, DK), BF16),
            V((RL * H * DK, 2 * DV), BF16),
            V((T, K, RL * H, DV), BF16),
            V((T, R, H, DV), F32),
            V((n, R, W), BF16),
            V((n, R, W), BF16),
            V((n, R, W), BF16),
            dma((14,)),
            dma,
            dma,
            dma((K,)),
            dma((K,)),
            dma((4, K)),
            dma((4, K)),
            dma((K, T)),
            dma((K, T)),
            dma((K, T)),
            dma((K, T)),
            dma((K, T)),
            dma((K, T)),
        ],
        compiler_params=pltpu.CompilerParams(
            collective_id=0, has_side_effects=True, vmem_limit_bytes=60 * 1024 * 1024
        ),
    )(*args)
    return pl.pallas_call(
        flush,
        out_shape=(
            jax.ShapeDtypeStruct((R, W), BF16),
            jax.ShapeDtypeStruct(past_state.shape, F32),
        ),
        in_specs=[pl.BlockSpec(memory_space=V)] * 2,
        out_specs=(anywhere,) * 2,
        scratch_shapes=[dma((2,))],
        compiler_params=pltpu.CompilerParams(vmem_limit_bytes=1024 * 1024),
    )(*outs)


def solution(mesh):
    placed = (
        P(("grp", "dp"), ("kv", "tp")),
        P(("grp", "dp", "kv"), "tp", None, None),
        P("kv"),
        P("kv", "tp"),
        P("kv", "tp"),
        P("kv", "tp"),
        P("kv", "tp"),
        P("tp"),
        P(),
        P(None, ("kv", "tp")),
        P(),
        P(None, ("kv", "tp")),
        P(None, ("kv", "tp")),
        P(("kv", "tp"), None),
    )
    return jax.shard_map(
        body,
        mesh=mesh,
        in_specs=placed,
        out_specs=(P(("grp", "dp"), ("kv", "tp")), P(("grp", "dp", "kv"), "tp", None, None)),
        check_vma=False,
    )
```

```python
import functools

import jax
import jax.numpy as jnp
from jax import lax
from jax.experimental import pallas as pl
from jax.experimental.pallas import tpu as pltpu
from jax.sharding import PartitionSpec as P

epsilon = 1e-06
F32 = jnp.float32
BF16 = jnp.bfloat16
MESH = pl.DeviceIdType.MESH


def sigmoid(a):
    return 1.0 / (1.0 + jnp.exp(-a))


def silu(a):
    return a / (1.0 + jnp.exp(-a))


def dot_t(a, b):
    return lax.dot_general(a, b, (((1,), (1,)), ((), ())), preferred_element_type=F32)


def kernel(
    K,
    T,
    tokens,
    past,
    mix_gain,
    w_query,
    w_forget,
    w_value,
    w_gate_out,
    floor_logits,
    head_gain,
    w_out,
    mlp_gain,
    w_gate,
    w_up,
    w_down,
    result,
    new_state,
    tok_v,
    past_v,
    mixg_v,
    proj_v,
    floor_v,
    hgain_v,
    wout_v,
    mlpg_v,
    wgate_v,
    wup_v,
    wdown_v,
    sq_send,
    sq_recv,
    part,
    part_send,
    part_recv,
    split_v,
    mix_all,
    mix_f,
    mid_all,
    term_send,
    term_recv,
    local_sem,
    tok_ss,
    tok_rs,
    sq_ss,
    sq_rs,
    part_ss,
    part_rs,
    wout_ss,
    wout_rs,
    mix_ss,
    mix_rs,
    mid_ss,
    mid_rs,
    term_ss,
    term_rs,
):
    R, W = tokens.shape
    RL, H, DK, DV = past.shape
    D = w_gate.shape[1]
    kv = lax.axis_index("kv")
    tp = lax.axis_index("tp")
    me = kv * T + tp

    hops = list(range(1, K))
    near = [(0, dt) for dt in range(1, T)] + [(j, dt) for j in hops for dt in range(T)]
    upper = (2 * kv) // K
    short = upper * (K - 1 - kv) + (1 - upper) * kv
    ahead = 1 - 2 * upper

    def hop(j):
        if j == 0:
            return kv
        both = jnp.minimum(jnp.maximum(2 * short - j + 1, 0), 1)
        step = both * ((j + 1) // 2) * (2 * (j % 2) - 1) + (1 - both) * (j - short)
        return kv + ahead * step

    def other(j, dt):
        return hop(j), (lax.rem(tp + dt, T) if j == 0 else dt)

    def source(j, dt):
        return hop(j), (lax.rem(tp + T - dt, T) if j == 0 else T - 1 - dt)

    def load(i, src, dst):
        copy = pltpu.make_async_copy(src, dst, local_sem.at[i])
        copy.start()
        return copy

    c_tok = load(0, tokens, tok_v.at[tp])
    c_mixg = load(1, mix_gain, mixg_v)
    c_proj = [
        load(2 + i, w, proj_v.at[i])
        for i, w in enumerate((w_forget, w_query, w_value, w_gate_out))
    ]
    c_past = load(6, past, past_v)
    c_floor = load(7, floor_logits, floor_v)
    c_hgain = load(8, head_gain, hgain_v)
    c_mlpg = load(9, mlp_gain, mlpg_v)

    barrier = pltpu.get_barrier_semaphore()

    def signal(k, t):
        pl.semaphore_signal(barrier, inc=1, device_id={"kv": k, "tp": t}, device_id_type=MESH)

    for j in hops[::-1]:
        signal(hop(j), 0)
    signal(kv, 1 - tp)
    c_tok.wait()

    def remote(src, dst, ss, rs, k, t):
        return pltpu.make_async_remote_copy(
            src_ref=src,
            dst_ref=dst,
            send_sem=ss,
            recv_sem=rs,
            device_id={"kv": k, "tp": t},
            device_id_type=MESH,
        )

    def send(*args):
        copy = remote(*args)
        copy.start()
        return copy

    def arrived(dst, ss, rs):
        pltpu.make_async_remote_copy(
            src_ref=dst,
            dst_ref=dst,
            send_sem=ss,
            recv_sem=rs,
            device_id={"kv": kv, "tp": lax.rem(tp + 1, T)},
            device_id_type=MESH,
        ).wait_recv()

    sent = []
    swap = pltpu.make_async_remote_copy(
        src_ref=tok_v.at[tp],
        dst_ref=tok_v.at[tp],
        send_sem=tok_ss,
        recv_sem=tok_rs,
        device_id={"kv": kv, "tp": 1 - tp},
        device_id_type=MESH,
    )
    sent.append(swap)

    @pl.when(tp == 1)
    def _():
        pl.semaphore_wait(barrier, 1)
        swap.start()

    c_mixg.wait()

    def features(t):
        block = tok_v[t].astype(F32)
        square = jnp.sum(block * block, axis=1, keepdims=True)
        rows = pl.ds(pl.multiple_of(t * W, W), W)
        return (block * mixg_v[t]).astype(BF16), rows, square

    def project(part_of, i):
        gained, rows, _ = part_of
        return jnp.dot(gained, proj_v[i, rows, :], preferred_element_type=F32)

    def spread_out(i, total):
        for h in range(H):
            part[i, :, h, :] = total[:, h * DK : (h + 1) * DK]
        for k in range(K):
            part_send[i, k] = part[i, k * RL : (k + 1) * RL].reshape(RL * H, DK).astype(BF16)

    def scatter(i):
        for j in hops[::-1]:
            k = hop(j)
            sent.append(
                send(
                    part_send.at[i, k],
                    part_recv.at[i, kv],
                    part_ss.at[i, j],
                    part_rs.at[i, kv],
                    k,
                    tp,
                )
            )

    mine = features(tp)
    early = []
    for i in range(2):
        c_proj[i].wait()
        early.append(project(mine, i))
    swap.wait_recv()
    theirs = features(1 - tp)
    square = jnp.broadcast_to(mine[2] + theirs[2], (R, DK))
    for k in range(K):
        sq_send[k] = square[k * RL : (k + 1) * RL]
    totals = [early[i] + project(theirs, i) for i in range(2)]
    spread_out(0, totals[0])
    spread_out(1, totals[1])

    @pl.when(tp == 0)
    def _():
        pl.semaphore_wait(barrier, K * T - 1)
        swap.start()

    for j in hops[::-1]:
        k = hop(j)
        sent.append(send(sq_send.at[k], sq_recv.at[kv], sq_ss.at[j], sq_rs.at[kv], k, tp))
    scatter(0)
    scatter(1)
    push = remote(w_out, wout_v.at[0], wout_ss, wout_rs, kv, 1)
    c_wgate = load(11, w_gate, wgate_v)
    c_wup = load(12, w_up, wup_v)
    c_wdown = load(13, w_down, wdown_v)
    totals = []
    for i in range(2, 4):
        c_proj[i].wait()
        totals.append(project(mine, i) + project(theirs, i))
    for i in range(2, 4):
        spread_out(i, totals[i - 2])
        scatter(i)

    @pl.when(tp == 0)
    def _():
        push.start()

    @pl.when(tp == 1)
    def _():
        pltpu.make_async_copy(w_out, wout_v.at[1], local_sem.at[10]).start()

    c_floor.wait()
    c_hgain.wait()
    lower = sigmoid(floor_v[...])
    lower = jnp.concatenate([lower] * RL, axis=0)
    c_past.wait()
    for s in range(RL):
        for h in range(H):
            rows = pl.ds((s * H + h) * DK, DK)
            block = past_v[s, h]
            high = block.astype(BF16)
            split_v[rows, :DV] = high
            split_v[rows, DV:] = (block - high.astype(F32)).astype(BF16)
    square = sq_send[kv]
    for dk in hops:
        k, t = source(dk, 0)
        arrived(sq_recv.at[k], sq_ss.at[dk], sq_rs.at[k])
        square = square + sq_recv[k]
    row_scale = lax.rsqrt(square / D + epsilon)
    row_scale = jnp.concatenate(
        [jnp.broadcast_to(row_scale[s : s + 1], (H, DK)) for s in range(RL)], axis=0
    )

    def summed(i):
        total = part[i, pl.ds(kv * RL, RL)].reshape(RL * H, DK)
        for dk in hops:
            k, t = source(dk, 0)
            arrived(part_recv.at[i, k], part_ss.at[i, dk], part_rs.at[i, k])
            total = total + part_recv[i, k].astype(F32)
        return total * row_scale

    forget = lower + (1.0 - lower) * sigmoid(summed(0))
    activ = silu(summed(1))
    weight = activ * forget
    high = weight.astype(BF16).astype(F32)
    weight = jnp.concatenate([high, weight - high], axis=0)
    owner = lax.rem(lax.broadcasted_iota(jnp.int32, weight.shape, 0), RL * H)
    left = jnp.concatenate(
        [jnp.where(owner == i, weight, 0.0).astype(BF16) for i in range(RL * H)], axis=1
    )
    wide = jnp.dot(left, split_v[...], preferred_element_type=F32)
    head_out = wide[: RL * H, :DV] + (wide[: RL * H, DV:] + wide[RL * H :, :DV])
    rest = jnp.sum(activ * (1.0 - forget), axis=1, keepdims=True)
    value = summed(2)
    head_out = head_out + value * rest
    normed = head_out * lax.rsqrt(
        jnp.mean(head_out * head_out, axis=1, keepdims=True) + epsilon
    )
    mixed = normed * hgain_v[...] * silu(summed(3))
    mix_all[tp, kv] = mixed.astype(BF16)
    slot = mix_all.at[tp, kv]
    for j in hops[::-1]:
        sent.append(send(slot, slot, mix_ss.at[j], mix_rs.at[kv, tp], hop(j), 1))
    aside = remote(slot, slot, mix_ss.at[0], mix_rs.at[kv, tp], kv, 1)

    @pl.when(tp == 0)
    def _():
        aside.start()

    columns = forget.T
    for s in range(RL):
        for h in range(H):
            i = s * H + h
            row = value[i : i + 1, :]
            new_state[s, h] = row + columns[:, i : i + 1] * (past_v[s, h] - row)

    def spread(t, k):
        mix_f[t, pl.ds(k * RL, RL)] = mix_all[t, k].astype(F32).reshape(RL, H, DV)

    given = []
    for t in range(T):
        slot = mid_all.at[kv * T + t]
        for j in hops[::-1] + [0]:
            for peer in range(1 if j == 0 else T):
                given.append(
                    remote(slot, slot, mid_ss.at[j, peer, t], mid_rs.at[kv, t], hop(j), peer)
                )

    @pl.when(tp == 1)
    def _():
        spread(1, kv)
        arrived(mix_all.at[0, kv], mix_ss.at[0], mix_rs.at[kv, 0])
        spread(0, kv)
        for j in hops:
            k = hop(j)
            for t in range(T)[::-1]:
                arrived(mix_all.at[t, k], mix_ss.at[j], mix_rs.at[k, t])
                spread(t, k)
        every_head = jnp.concatenate(
            [mix_f[t, :, h, :].astype(BF16) for t in range(T) for h in range(H)], axis=1
        )
        pltpu.make_async_copy(w_out, wout_v.at[1], local_sem.at[10]).wait()
        arrived(wout_v.at[0], wout_ss, wout_rs)
        for t in range(T):
            middle = tok_v[t].astype(F32) + jnp.dot(
                every_head, wout_v[t], preferred_element_type=F32
            )
            mid_all[kv * T + t] = middle.astype(BF16)
            for copy in given[t * len(given) // T : (t + 1) * len(given) // T]:
                copy.start()

    c_mlpg.wait()
    square = jnp.zeros((R, 1), F32)
    gate = None
    if W % 128 == 0:
        groups = [[(j, t)] for j in [0] + hops for t in range(T)]
    else:
        groups = [[(j, t) for t in range(T)] for j in [0] + hops]
    for group in groups:
        k = hop(group[0][0])
        for j, t in group:
            if j:
                arrived(mid_all.at[k * T + t], mid_ss.at[j, 0, t], mid_rs.at[k, t])
            else:

                @pl.when(tp == 0)
                def _(t=t):
                    arrived(mid_all.at[kv * T + t], mid_ss.at[0, 0, t], mid_rs.at[kv, t])

        j = k * T + group[0][1]
        blocks = []
        for i in range(len(group)):
            block = mid_all[j + i].astype(F32)
            square = square + jnp.sum(block * block, axis=1, keepdims=True)
            blocks.append((block * mlpg_v[j + i]).astype(BF16))
        block = jnp.concatenate(blocks, axis=1) if len(blocks) > 1 else blocks[0]
        width = len(group) * W
        lanes = pl.ds(pl.multiple_of(j * W, width), width)
        if gate is None:
            c_wgate.wait()
        g = dot_t(block, wgate_v[:, lanes])
        if gate is None:
            c_wup.wait()
        u = dot_t(block, wup_v[:, lanes])
        gate, upward = (g, u) if gate is None else (gate + g, upward + u)
    mlp_scale = lax.rsqrt(square / D + epsilon)
    hidden = (silu(gate * mlp_scale) * (upward * mlp_scale)).astype(BF16)
    c_wdown.wait()
    for dk in hops[::-1] + [0]:
        k, _ = other(dk, 0)
        lanes = pl.ds(pl.multiple_of(k * T * W, T * W), T * W)
        chunk = jnp.dot(hidden, wdown_v[:, lanes], preferred_element_type=F32).astype(BF16)
        for t in range(T):
            term_send[k * T + t] = chunk[:, t * W : (t + 1) * W]
        for dt in range(0 if dk else 1, T):
            _, t = other(dk, dt)
            sent.append(
                send(
                    term_send.at[k * T + t],
                    term_recv.at[me],
                    term_ss.at[dk, dt],
                    term_rs.at[kv, tp],
                    k,
                    t,
                )
            )
    total = term_send[me].astype(F32)
    for dk, dt in near:
        k, t = source(dk, dt)
        j = k * T + t
        arrived(term_recv.at[j], term_ss.at[dk, dt], term_rs.at[k, t])
        total = total + term_recv[j].astype(F32)
    result[...] = (mid_all[me].astype(F32) + total).astype(BF16)
    for copy in sent:
        copy.wait_send()

    @pl.when(tp == 0)
    def _():
        push.wait_send()
        aside.wait_send()

    @pl.when(tp == 1)
    def _():
        for copy in given:
            copy.wait_send()


def flush(result_v, state_v, result, new_state, sem):
    copies = [
        pltpu.make_async_copy(state_v, new_state, sem.at[0]),
        pltpu.make_async_copy(result_v, result, sem.at[1]),
    ]
    for copy in copies:
        copy.start()
    for copy in copies:
        copy.wait()


def body(
    tokens,
    past_state,
    mix_gain,
    w_query,
    w_forget,
    w_value,
    w_gate_out,
    floor_logits,
    head_gain,
    w_out,
    mlp_gain,
    w_gate,
    w_up,
    w_down,
):
    K = lax.axis_size("kv")
    T = lax.axis_size("tp")
    assert T == 2
    n = K * T
    R, W = tokens.shape
    RL, H, DK, DV = past_state.shape
    args = (
        tokens,
        past_state,
        mix_gain.reshape(T, 1, W),
        w_query,
        w_forget,
        w_value,
        w_gate_out,
        floor_logits.reshape(H, DK),
        head_gain.reshape(1, DV),
        w_out,
        mlp_gain.reshape(n, 1, W),
        w_gate.T,
        w_up.T,
        w_down,
    )
    V = pltpu.VMEM
    dma = pltpu.SemaphoreType.DMA
    anywhere = pl.BlockSpec(memory_space=pl.ANY)
    outs = pl.pallas_call(
        functools.partial(kernel, K, T),
        out_shape=(
            pltpu.VMEM((R, W), BF16),
            pltpu.VMEM(past_state.shape, F32),
        ),
        in_specs=[anywhere] * len(args),
        out_specs=(pl.BlockSpec(memory_space=pltpu.VMEM),)*2,
        scratch_shapes=[
            V((T, R, W), BF16),
            V(past_state.shape, F32),
            V((T, 1, W), F32),
            V((4,) + w_query.shape, BF16),
            V((H, DK), F32),
            V((1, DV), F32),
            V((T,) + w_out.shape, BF16),
            V((n, 1, W), F32),
            V(w_gate.shape[::-1], BF16),
            V(w_up.shape[::-1], BF16),
            V(w_down.shape, BF16),
            V((K, RL, DK), F32),
            V((K, RL, DK), F32),
            V((4, R, H, DK), F32),
            V((4, K, RL * H, DK), BF16),
            V((4, K, RL * H, DK), BF16),
            V((RL * H * DK, 2 * DV), BF16),
            V((T, K, RL * H, DV), BF16),
            V((T, R, H, DV), F32),
            V((n, R, W), BF16),
            V((n, R, W), BF16),
            V((n, R, W), BF16),
            dma((14,)),
            dma,
            dma,
            dma((K,)),
            dma((K,)),
            dma((4, K)),
            dma((4, K)),
            dma,
            dma,
            dma((K,)),
            dma((K, T)),
            dma((K, T, T)),
            dma((K, T)),
            dma((K, T)),
            dma((K, T)),
        ],
        compiler_params=pltpu.CompilerParams(
            collective_id=0, has_side_effects=True, vmem_limit_bytes=60 * 1024 * 1024
        ),
    )(*args)
    return pl.pallas_call(
        flush,
        out_shape=(
            jax.ShapeDtypeStruct((R, W), BF16),
            jax.ShapeDtypeStruct(past_state.shape, F32),
        ),
        in_specs=[pl.BlockSpec(memory_space=V)] * 2,
        out_specs=(anywhere,) * 2,
        scratch_shapes=[dma((2,))],
        compiler_params=pltpu.CompilerParams(vmem_limit_bytes=1024 * 1024),
    )(*outs)


def solution(mesh):
    placed = (
        P(("grp", "dp"), ("kv", "tp")),
        P(("grp", "dp", "kv"), "tp", None, None),
        P("kv"),
        P("kv", "tp"),
        P("kv", "tp"),
        P("kv", "tp"),
        P("kv", "tp"),
        P("tp"),
        P(),
        P(None, ("kv", "tp")),
        P(),
        P(None, ("kv", "tp")),
        P(None, ("kv", "tp")),
        P(("kv", "tp"), None),
    )
    return jax.shard_map(
        body,
        mesh=mesh,
        in_specs=placed,
        out_specs=(P(("grp", "dp"), ("kv", "tp")), P(("grp", "dp", "kv"), "tp", None, None)),
        check_vma=False,
    )
```

```python
import functools

import jax
import jax.numpy as jnp
from jax import lax
from jax.experimental import pallas as pl
from jax.experimental.pallas import tpu as pltpu
from jax.sharding import PartitionSpec as P

epsilon = 1e-06
F32 = jnp.float32
BF16 = jnp.bfloat16
MESH = pl.DeviceIdType.MESH


def sigmoid(a):
    return 1.0 / (1.0 + jnp.exp(-a))


def silu(a):
    return a / (1.0 + jnp.exp(-a))


def dot_t(a, b):
    return lax.dot_general(a, b, (((1,), (1,)), ((), ())), preferred_element_type=F32)


def kernel(
    K,
    T,
    tokens,
    past,
    mix_gain,
    w_query,
    w_forget,
    w_value,
    w_gate_out,
    floor_logits,
    head_gain,
    w_out,
    mlp_gain,
    w_gate,
    w_up,
    w_down,
    result,
    new_state,
    tok_v,
    past_v,
    mixg_v,
    proj_v,
    floor_v,
    hgain_v,
    wout_v,
    mlpg_v,
    wgate_v,
    wup_v,
    wdown_v,
    sq_send,
    sq_recv,
    part,
    part_send,
    part_recv,
    round_v,
    mix_all,
    mix_f,
    mid_all,
    term_send,
    term_recv,
    local_sem,
    ready,
    tok_ss,
    tok_rs,
    sq_ss,
    sq_rs,
    part_ss,
    part_rs,
    again_ss,
    floor_ss,
    floor_rs,
    past_ss,
    past_rs,
    wout_ss,
    wout_rs,
    mix_ss,
    mix_rs,
    mid_ss,
    mid_rs,
    term_ss,
    term_rs,
):
    R, W = tokens.shape
    RL, H, DK, DV = past.shape
    D = w_gate.shape[1]
    kv = lax.axis_index("kv")
    tp = lax.axis_index("tp")
    me = kv * T + tp

    hops = list(range(1, K))
    near = [(0, dt) for dt in range(1, T)] + [(j, dt) for j in hops for dt in range(T)]
    upper = (2 * kv) // K
    short = upper * (K - 1 - kv) + (1 - upper) * kv
    ahead = 1 - 2 * upper

    def hop(j):
        if j == 0:
            return kv
        both = jnp.minimum(jnp.maximum(2 * short - j + 1, 0), 1)
        step = both * ((j + 1) // 2) * (2 * (j % 2) - 1) + (1 - both) * (j - short)
        return kv + ahead * step

    def other(j, dt):
        return hop(j), (lax.rem(tp + dt, T) if j == 0 else dt)

    def source(j, dt):
        return hop(j), (lax.rem(tp + T - dt, T) if j == 0 else T - 1 - dt)

    def load(i, src, dst):
        copy = pltpu.make_async_copy(src, dst, local_sem.at[i])
        copy.start()
        return copy

    c_tok = load(0, tokens, tok_v.at[tp])
    c_mixg = load(1, mix_gain, mixg_v)
    c_proj = [
        load(2 + i, w, proj_v.at[i])
        for i, w in enumerate((w_forget, w_query, w_value, w_gate_out))
    ]
    c_past = load(6, past, past_v)
    c_floor = load(7, floor_logits, floor_v.at[tp])
    c_hgain = load(8, head_gain, hgain_v)
    c_mlpg = load(9, mlp_gain, mlpg_v)

    barrier = pltpu.get_barrier_semaphore()

    def signal(k, t):
        pl.semaphore_signal(barrier, inc=1, device_id={"kv": k, "tp": t}, device_id_type=MESH)

    for j in hops[::-1]:
        signal(hop(j), 0)

    @pl.when(tp == 0)
    def _():
        signal(kv, 1)

    c_tok.wait()

    def remote(src, dst, ss, rs, k, t):
        return pltpu.make_async_remote_copy(
            src_ref=src,
            dst_ref=dst,
            send_sem=ss,
            recv_sem=rs,
            device_id={"kv": k, "tp": t},
            device_id_type=MESH,
        )

    def send(*args):
        copy = remote(*args)
        copy.start()
        return copy

    def arrived(dst, ss, rs):
        pltpu.make_async_remote_copy(
            src_ref=dst,
            dst_ref=dst,
            send_sem=ss,
            recv_sem=rs,
            device_id={"kv": kv, "tp": lax.rem(tp + 1, T)},
            device_id_type=MESH,
        ).wait_recv()

    sent = []
    swap = pltpu.make_async_remote_copy(
        src_ref=tok_v.at[tp],
        dst_ref=tok_v.at[tp],
        send_sem=tok_ss,
        recv_sem=tok_rs,
        device_id={"kv": kv, "tp": 1 - tp},
        device_id_type=MESH,
    )
    sent.append(swap)

    @pl.when(tp == 1)
    def _():
        pl.semaphore_wait(barrier, 1)
        pl.semaphore_signal(ready, inc=1, device_id={"kv": kv, "tp": 0}, device_id_type=MESH)
        swap.start()

    @pl.when(tp == 0)
    def _():
        pl.semaphore_wait(ready, 1)
        swap.start()

    c_mixg.wait()

    def features(t):
        block = tok_v[t].astype(F32)
        square = jnp.sum(block * block, axis=1, keepdims=True)
        rows = pl.ds(pl.multiple_of(t * W, W), W)
        return (block * mixg_v[t]).astype(BF16), rows, square

    def project(part_of, i):
        gained, rows, _ = part_of
        return jnp.dot(gained, proj_v[i, rows, :], preferred_element_type=F32)

    def spread_out(i, total):
        for h in range(H):
            part[i, :, h, :] = total[:, h * DK : (h + 1) * DK]
        for k in range(K):
            part_send[i, k] = part[i, k * RL : (k + 1) * RL].reshape(RL * H, DK).astype(BF16)

    def scatter(i):
        for j in hops[::-1]:
            k = hop(j)
            sent.append(
                send(
                    part_send.at[i, k],
                    part_recv.at[tp, i, kv],
                    part_ss.at[i, j],
                    part_rs.at[tp, i, kv],
                    k,
                    1,
                )
            )
        own = remote(
            part_send.at[i, kv],
            part_recv.at[0, i, kv],
            part_ss.at[i, 0],
            part_rs.at[0, i, kv],
            kv,
            1,
        )
        from_zero.append(own)

        @pl.when(tp == 0)
        def _():
            own.start()

    from_zero = []
    mine = features(tp)
    swap.wait_recv()
    theirs = features(1 - tp)
    square = jnp.broadcast_to(mine[2] + theirs[2], (R, DK))
    for k in range(K):
        sq_send[k] = square[k * RL : (k + 1) * RL]
    totals = []
    for i in range(2):
        c_proj[i].wait()
        totals.append(project(mine, i) + project(theirs, i))
    spread_out(0, totals[0])
    spread_out(1, totals[1])

    @pl.when(tp == 0)
    def _():
        pl.semaphore_wait(barrier, (K - 1) * T)
        pl.semaphore_signal(ready, inc=1, device_id={"kv": kv, "tp": 1}, device_id_type=MESH)

    @pl.when(tp == 1)
    def _():
        pl.semaphore_wait(ready, 1)

    for j in hops[::-1]:
        k = hop(j)
        sent.append(send(sq_send.at[k], sq_recv.at[kv], sq_ss.at[j], sq_rs.at[kv], k, tp))
    scatter(0)
    scatter(1)
    push = remote(w_out, wout_v.at[0], wout_ss, wout_rs, kv, 1)
    c_wgate = load(11, w_gate, wgate_v)
    c_wup = load(12, w_up, wup_v)
    c_wdown = load(13, w_down, wdown_v)
    totals = []
    for i in range(2, 4):
        c_proj[i].wait()
        totals.append(project(mine, i) + project(theirs, i))
    for i in range(2, 4):
        spread_out(i, totals[i - 2])
        scatter(i)

    for i in (0, 2):
        for j in hops[::-1]:
            k = hop(j)
            from_zero.append(
                remote(
                    part_send.at[i, k],
                    part_recv.at[0, i, kv],
                    again_ss.at[i // 2, j],
                    part_rs.at[0, i, kv],
                    k,
                    0,
                )
            )
    c_past.wait()
    for s in range(RL):
        for h in range(H):
            rows = pl.ds((s * H + h) * DK, DK)
            round_v[tp, rows, :] = past_v[s, h].astype(BF16)
    pushes = [
        remote(floor_logits, floor_v.at[0], floor_ss, floor_rs, kv, 1),
        remote(round_v.at[0], round_v.at[0], past_ss, past_rs, kv, 1),
        push,
    ]

    @pl.when(tp == 0)
    def _():
        for copy in pushes[:2] + from_zero[4:] + pushes[2:]:
            copy.start()

    @pl.when(tp == 1)
    def _():
        pltpu.make_async_copy(w_out, wout_v.at[1], local_sem.at[10]).start()

    c_floor.wait()
    c_hgain.wait()
    square = sq_send[kv]
    for dk in hops:
        k, t = source(dk, 0)
        arrived(sq_recv.at[k], sq_ss.at[dk], sq_rs.at[k])
        square = square + sq_recv[k]
    row_scale = lax.rsqrt(square / D + epsilon)
    row_scale = jnp.concatenate(
        [jnp.broadcast_to(row_scale[s : s + 1], (H, DK)) for s in range(RL)], axis=0
    )

    def own_part(i):
        return part[i, pl.ds(kv * RL, RL)].reshape(RL * H, DK)

    def from_peers(u, i):
        for j in hops:
            k = hop(j)
            arrived(part_recv.at[u, i, k], part_ss.at[i, j], part_rs.at[u, i, k])

    def summed(u, i, total):
        for j in hops:
            total = total + part_recv[u, i, hop(j)].astype(F32)
        return total * row_scale

    def from_zeros(i):
        arrived(part_recv.at[0, i, kv], part_ss.at[i, 0], part_rs.at[0, i, kv])
        from_peers(0, i)

    def total_of(u, i):
        own = part_recv[0, i, kv].astype(F32) if u == 0 else own_part(i)
        return summed(u, i, own)

    def forget_of(u, total):
        lower = sigmoid(floor_v[u])
        lower = jnp.concatenate([lower] * RL, axis=0)
        return lower + (1.0 - lower) * sigmoid(total)

    owner = lax.broadcasted_iota(jnp.int32, (RL * H, DK), 0)

    def weighted(u, forget, activ):
        weight = activ * forget
        left = jnp.concatenate(
            [jnp.where(owner == i, weight, 0.0).astype(BF16) for i in range(RL * H)], axis=1
        )
        return (
            jnp.dot(left, round_v[u], preferred_element_type=F32),
            jnp.sum(activ * (1.0 - forget), axis=1, keepdims=True),
        )

    def gated(u, head_out, gate_pre):
        normed = head_out * lax.rsqrt(
            jnp.mean(head_out * head_out, axis=1, keepdims=True) + epsilon
        )
        mix_all[kv, u] = (normed * hgain_v[...] * silu(gate_pre)).astype(BF16)

    from_peers(tp, 0)
    forget = forget_of(tp, summed(tp, 0, own_part(0)))
    mix_sends = [
        remote(mix_all.at[kv], mix_all.at[kv], mix_ss.at[j], mix_rs.at[kv], hop(j), 1)
        for j in hops[::-1]
    ]

    @pl.when(tp == 0)
    def _():
        from_peers(0, 2)

    @pl.when(tp == 1)
    def _():
        arrived(floor_v.at[0], floor_ss, floor_rs)
        arrived(round_v.at[0], past_ss, past_rs)
        from_zeros(0)
        from_zeros(1)
        from_peers(1, 1)
        zero, zero_rest = weighted(0, forget_of(0, total_of(0, 0)), silu(total_of(0, 1)))
        one, one_rest = weighted(1, forget, silu(total_of(1, 1)))
        for i in (2, 3):
            from_zeros(i)
            from_peers(1, i)
        gated(0, zero + total_of(0, 2) * zero_rest, total_of(0, 3))
        gated(1, one + total_of(1, 2) * one_rest, total_of(1, 3))
        for copy in mix_sends:
            copy.start()

    value = summed(tp, 2, own_part(2))
    columns = forget.T
    for s in range(RL):
        for h in range(H):
            i = s * H + h
            row = value[i : i + 1, :]
            new_state[s, h] = row + columns[:, i : i + 1] * (past_v[s, h] - row)

    def spread(t, k):
        mix_f[t, pl.ds(k * RL, RL)] = mix_all[k, t].astype(F32).reshape(RL, H, DV)

    given = []
    for t in range(T):
        slot = mid_all.at[kv * T + t]
        for j in hops[::-1] + [0]:
            for peer in range(1 if j == 0 else T):
                given.append(
                    remote(slot, slot, mid_ss.at[j, peer, t], mid_rs.at[kv, t], hop(j), peer)
                )

    @pl.when(tp == 1)
    def _():
        for j in [0] + hops:
            k = hop(j)
            if j:
                arrived(mix_all.at[k], mix_ss.at[j], mix_rs.at[k])
            for t in range(T):
                spread(t, k)
        every_head = jnp.concatenate(
            [mix_f[t, :, h, :].astype(BF16) for t in range(T) for h in range(H)], axis=1
        )
        pltpu.make_async_copy(w_out, wout_v.at[1], local_sem.at[10]).wait()
        arrived(wout_v.at[0], wout_ss, wout_rs)
        for t in range(T):
            middle = tok_v[t].astype(F32) + jnp.dot(
                every_head, wout_v[t], preferred_element_type=F32
            )
            mid_all[kv * T + t] = middle.astype(BF16)
            for copy in given[t * len(given) // T : (t + 1) * len(given) // T]:
                copy.start()

    c_mlpg.wait()
    square = jnp.zeros((R, 1), F32)
    gate = None
    if W % 128 == 0:
        groups = [[(j, t)] for j in [0] + hops for t in range(T)]
    else:
        groups = [[(j, t) for t in range(T)] for j in [0] + hops]
    for group in groups:
        k = hop(group[0][0])
        for j, t in group:
            if j:
                arrived(mid_all.at[k * T + t], mid_ss.at[j, 0, t], mid_rs.at[k, t])
            else:

                @pl.when(tp == 0)
                def _(t=t):
                    arrived(mid_all.at[kv * T + t], mid_ss.at[0, 0, t], mid_rs.at[kv, t])

        j = k * T + group[0][1]
        blocks = []
        for i in range(len(group)):
            block = mid_all[j + i].astype(F32)
            square = square + jnp.sum(block * block, axis=1, keepdims=True)
            blocks.append((block * mlpg_v[j + i]).astype(BF16))
        block = jnp.concatenate(blocks, axis=1) if len(blocks) > 1 else blocks[0]
        width = len(group) * W
        lanes = pl.ds(pl.multiple_of(j * W, width), width)
        if gate is None:
            c_wgate.wait()
        g = dot_t(block, wgate_v[:, lanes])
        if gate is None:
            c_wup.wait()
        u = dot_t(block, wup_v[:, lanes])
        gate, upward = (g, u) if gate is None else (gate + g, upward + u)
    mlp_scale = lax.rsqrt(square / D + epsilon)
    hidden = (silu(gate * mlp_scale) * (upward * mlp_scale)).astype(BF16)
    c_wdown.wait()
    for dk in hops[::-1] + [0]:
        k, _ = other(dk, 0)
        lanes = pl.ds(pl.multiple_of(k * T * W, T * W), T * W)
        chunk = jnp.dot(hidden, wdown_v[:, lanes], preferred_element_type=F32).astype(BF16)
        for t in range(T):
            term_send[k * T + t] = chunk[:, t * W : (t + 1) * W]
        for dt in range(0 if dk else 1, T):
            _, t = other(dk, dt)
            sent.append(
                send(
                    term_send.at[k * T + t],
                    term_recv.at[me],
                    term_ss.at[dk, dt],
                    term_rs.at[kv, tp],
                    k,
                    t,
                )
            )
    total = term_send[me].astype(F32)
    for dk, dt in near:
        k, t = source(dk, dt)
        j = k * T + t
        arrived(term_recv.at[j], term_ss.at[dk, dt], term_rs.at[k, t])
        total = total + term_recv[j].astype(F32)
    result[...] = (mid_all[me].astype(F32) + total).astype(BF16)
    for copy in sent:
        copy.wait_send()

    @pl.when(tp == 0)
    def _():
        for copy in from_zero + pushes:
            copy.wait_send()

    @pl.when(tp == 1)
    def _():
        for copy in mix_sends + given:
            copy.wait_send()


def flush(result_v, state_v, result, new_state, sem):
    copies = [
        pltpu.make_async_copy(state_v, new_state, sem.at[0]),
        pltpu.make_async_copy(result_v, result, sem.at[1]),
    ]
    for copy in copies:
        copy.start()
    for copy in copies:
        copy.wait()


def body(
    tokens,
    past_state,
    mix_gain,
    w_query,
    w_forget,
    w_value,
    w_gate_out,
    floor_logits,
    head_gain,
    w_out,
    mlp_gain,
    w_gate,
    w_up,
    w_down,
):
    K = lax.axis_size("kv")
    T = lax.axis_size("tp")
    assert T == 2
    n = K * T
    R, W = tokens.shape
    RL, H, DK, DV = past_state.shape
    args = (
        tokens,
        past_state,
        mix_gain.reshape(T, 1, W),
        w_query,
        w_forget,
        w_value,
        w_gate_out,
        floor_logits.reshape(H, DK),
        head_gain.reshape(1, DV),
        w_out,
        mlp_gain.reshape(n, 1, W),
        w_gate.T,
        w_up.T,
        w_down,
    )
    V = pltpu.VMEM
    dma = pltpu.SemaphoreType.DMA
    anywhere = pl.BlockSpec(memory_space=pl.ANY)
    outs = pl.pallas_call(
        functools.partial(kernel, K, T),
        out_shape=(
            pltpu.VMEM((R, W), BF16),
            pltpu.VMEM(past_state.shape, F32),
        ),
        in_specs=[anywhere] * len(args),
        out_specs=(pl.BlockSpec(memory_space=pltpu.VMEM),)*2,
        scratch_shapes=[
            V((T, R, W), BF16),
            V(past_state.shape, F32),
            V((T, 1, W), F32),
            V((4,) + w_query.shape, BF16),
            V((T, H, DK), F32),
            V((1, DV), F32),
            V((T,) + w_out.shape, BF16),
            V((n, 1, W), F32),
            V(w_gate.shape[::-1], BF16),
            V(w_up.shape[::-1], BF16),
            V(w_down.shape, BF16),
            V((K, RL, DK), F32),
            V((K, RL, DK), F32),
            V((4, R, H, DK), F32),
            V((4, K, RL * H, DK), BF16),
            V((T, 4, K, RL * H, DK), BF16),
            V((T, RL * H * DK, DV), BF16),
            V((K, T, RL * H, DV), BF16),
            V((T, R, H, DV), F32),
            V((n, R, W), BF16),
            V((n, R, W), BF16),
            V((n, R, W), BF16),
            dma((14,)),
            pltpu.SemaphoreType.REGULAR,
            dma,
            dma,
            dma((K,)),
            dma((K,)),
            dma((4, K)),
            dma((T, 4, K)),
            dma((2, K)),
            dma,
            dma,
            dma,
            dma,
            dma,
            dma,
            dma((K,)),
            dma((K,)),
            dma((K, T, T)),
            dma((K, T)),
            dma((K, T)),
            dma((K, T)),
        ],
        compiler_params=pltpu.CompilerParams(
            collective_id=0, has_side_effects=True, vmem_limit_bytes=60 * 1024 * 1024
        ),
    )(*args)
    return pl.pallas_call(
        flush,
        out_shape=(
            jax.ShapeDtypeStruct((R, W), BF16),
            jax.ShapeDtypeStruct(past_state.shape, F32),
        ),
        in_specs=[pl.BlockSpec(memory_space=V)] * 2,
        out_specs=(anywhere,) * 2,
        scratch_shapes=[dma((2,))],
        compiler_params=pltpu.CompilerParams(vmem_limit_bytes=1024 * 1024),
    )(*outs)


def solution(mesh):
    placed = (
        P(("grp", "dp"), ("kv", "tp")),
        P(("grp", "dp", "kv"), "tp", None, None),
        P("kv"),
        P("kv", "tp"),
        P("kv", "tp"),
        P("kv", "tp"),
        P("kv", "tp"),
        P("tp"),
        P(),
        P(None, ("kv", "tp")),
        P(),
        P(None, ("kv", "tp")),
        P(None, ("kv", "tp")),
        P(("kv", "tp"), None),
    )
    return jax.shard_map(
        body,
        mesh=mesh,
        in_specs=placed,
        out_specs=(P(("grp", "dp"), ("kv", "tp")), P(("grp", "dp", "kv"), "tp", None, None)),
        check_vma=False,
    )
```

```python
import functools

import jax
import jax.numpy as jnp
from jax import lax
from jax.experimental import pallas as pl
from jax.experimental.pallas import tpu as pltpu
from jax.sharding import PartitionSpec as P

epsilon = 1e-06
F32 = jnp.float32
BF16 = jnp.bfloat16
MESH = pl.DeviceIdType.MESH


def sigmoid(a):
    return 1.0 / (1.0 + jnp.exp(-a))


def silu(a):
    return a / (1.0 + jnp.exp(-a))


def kernel(
    K,
    T,
    tokens,
    past,
    mix_gain,
    w_query,
    w_forget,
    w_value,
    w_gate_out,
    floor_logits,
    head_gain,
    w_out,
    mlp_gain,
    w_gate,
    w_up,
    w_down,
    result,
    new_state,
    tok_v,
    past_v,
    mixg_v,
    proj_v,
    floor_v,
    hgain_v,
    wout_v,
    mlpg_v,
    wgate_v,
    wup_v,
    gatet_v,
    upt_v,
    wdown_v,
    sq_send,
    sq_recv,
    part,
    part_send,
    part_recv,
    round_v,
    mix_all,
    mix_f,
    mid_all,
    term_send,
    term_recv,
    local_sem,
    ready,
    tok_ss,
    tok_rs,
    sq_ss,
    sq_rs,
    part_ss,
    part_rs,
    again_ss,
    floor_ss,
    floor_rs,
    past_ss,
    past_rs,
    wout_ss,
    wout_rs,
    mix_ss,
    mix_rs,
    mid_ss,
    mid_rs,
    term_ss,
    term_rs,
):
    R, W = tokens.shape
    RL, H, DK, DV = past.shape
    D = w_gate.shape[1]
    kv = lax.axis_index("kv")
    tp = lax.axis_index("tp")
    me = kv * T + tp

    hops = list(range(1, K))
    near = [(0, dt) for dt in range(1, T)] + [(j, dt) for j in hops for dt in range(T)]
    upper = (2 * kv) // K
    short = upper * (K - 1 - kv) + (1 - upper) * kv
    ahead = 1 - 2 * upper

    def hop(j):
        if j == 0:
            return kv
        both = jnp.minimum(jnp.maximum(2 * short - j + 1, 0), 1)
        step = both * ((j + 1) // 2) * (2 * (j % 2) - 1) + (1 - both) * (j - short)
        return kv + ahead * step

    def other(j, dt):
        return hop(j), (lax.rem(tp + dt, T) if j == 0 else dt)

    def source(j, dt):
        return hop(j), (lax.rem(tp + T - dt, T) if j == 0 else T - 1 - dt)

    def load(i, src, dst):
        copy = pltpu.make_async_copy(src, dst, local_sem.at[i])
        copy.start()
        return copy

    c_tok = load(0, tokens, tok_v.at[tp])
    c_mixg = load(1, mix_gain, mixg_v)
    c_proj = [
        load(2 + i, w, proj_v.at[i])
        for i, w in enumerate((w_forget, w_query, w_value, w_gate_out))
    ]
    c_past = load(6, past, past_v)
    c_floor = load(7, floor_logits, floor_v.at[tp])
    c_hgain = load(8, head_gain, hgain_v)
    c_mlpg = load(9, mlp_gain, mlpg_v)

    barrier = pltpu.get_barrier_semaphore()

    def signal(k, t):
        pl.semaphore_signal(barrier, inc=1, device_id={"kv": k, "tp": t}, device_id_type=MESH)

    for j in hops[::-1]:
        signal(hop(j), 0)

    @pl.when(tp == 0)
    def _():
        signal(kv, 1)

    @pl.when(tp == 1)
    def _():
        pl.semaphore_wait(barrier, 1)
        pl.semaphore_signal(ready, inc=1, device_id={"kv": kv, "tp": 0}, device_id_type=MESH)

    c_tok.wait()

    def remote(src, dst, ss, rs, k, t):
        return pltpu.make_async_remote_copy(
            src_ref=src,
            dst_ref=dst,
            send_sem=ss,
            recv_sem=rs,
            device_id={"kv": k, "tp": t},
            device_id_type=MESH,
        )

    def send(*args):
        copy = remote(*args)
        copy.start()
        return copy

    def arrived(dst, ss, rs):
        pltpu.make_async_remote_copy(
            src_ref=dst,
            dst_ref=dst,
            send_sem=ss,
            recv_sem=rs,
            device_id={"kv": kv, "tp": lax.rem(tp + 1, T)},
            device_id_type=MESH,
        ).wait_recv()

    def left(src, ss):
        pltpu.make_async_remote_copy(
            src_ref=src,
            dst_ref=src,
            send_sem=ss,
            recv_sem=tok_rs,
            device_id={"kv": kv, "tp": 1 - tp},
            device_id_type=MESH,
        ).wait_send()

    most = pl.ds(0, K - 1)
    swap = pltpu.make_async_remote_copy(
        src_ref=tok_v.at[tp],
        dst_ref=tok_v.at[tp],
        send_sem=tok_ss,
        recv_sem=tok_rs,
        device_id={"kv": kv, "tp": 1 - tp},
        device_id_type=MESH,
    )

    @pl.when(tp == 0)
    def _():
        pl.semaphore_wait(ready, 1)

    swap.start()
    c_mixg.wait()

    def features(t):
        block = tok_v[t].astype(F32)
        square = jnp.sum(block * block, axis=1, keepdims=True)
        rows = pl.ds(pl.multiple_of(t * W, W), W)
        return (block * mixg_v[t]).astype(BF16), rows, square

    def project(part_of, i):
        gained, rows, _ = part_of
        return jnp.dot(gained, proj_v[i, rows, :], preferred_element_type=F32)

    def spread_out(i, total):
        for h in range(H):
            part[i, :, h, :] = total[:, h * DK : (h + 1) * DK]
        for k in range(K):
            part_send[i, k] = part[i, k * RL : (k + 1) * RL].reshape(RL * H, DK).astype(BF16)

    def scatter(i):
        for j in hops[::-1]:
            k = hop(j)
            send(
                part_send.at[i, k],
                part_recv.at[tp, i, kv],
                part_ss,
                part_rs.at[tp, i // 2],
                k,
                1,
            )
        own = remote(
            part_send.at[i, kv],
            part_recv.at[0, i, kv],
            part_ss,
            part_rs.at[0, i // 2],
            kv,
            1,
        )

        @pl.when(tp == 0)
        def _():
            own.start()

    again = []
    mine = features(tp)
    early = []
    for i in range(2):
        c_proj[i].wait()
        early.append(project(mine, i))
    swap.wait_recv()
    theirs = features(1 - tp)
    square = jnp.broadcast_to(mine[2] + theirs[2], (R, DK))
    for k in range(K):
        sq_send[k] = square[k * RL : (k + 1) * RL]
    totals = [early[i] + project(theirs, i) for i in range(2)]
    spread_out(0, totals[0])
    spread_out(1, totals[1])

    @pl.when(tp == 0)
    def _():
        pl.semaphore_wait(barrier, (K - 1) * T)
        pl.semaphore_signal(ready, inc=1, device_id={"kv": kv, "tp": 1}, device_id_type=MESH)

    @pl.when(tp == 1)
    def _():
        pl.semaphore_wait(ready, 1)

    for j in hops[::-1]:
        k = hop(j)
        send(sq_send.at[k], sq_recv.at[kv], sq_ss, sq_rs, k, tp)
    scatter(0)
    scatter(1)
    push = remote(w_out, wout_v.at[0], wout_ss, wout_rs, kv, 1)
    c_wgate = load(11, w_gate, wgate_v)
    c_wup = load(12, w_up, wup_v)
    c_wdown = load(13, w_down, wdown_v)
    totals = []
    for i in range(2, 4):
        c_proj[i].wait()
        totals.append(project(mine, i) + project(theirs, i))
    for i in range(2, 4):
        spread_out(i, totals[i - 2])
        scatter(i)

    for i in (0, 2):
        for j in hops[::-1]:
            k = hop(j)
            again.append(
                remote(
                    part_send.at[i, k],
                    part_recv.at[0, i, kv],
                    again_ss,
                    part_rs.at[0, i // 2],
                    k,
                    0,
                )
            )
    c_past.wait()
    for s in range(RL):
        for h in range(H):
            rows = pl.ds((s * H + h) * DK, DK)
            round_v[tp, rows, :] = past_v[s, h].astype(BF16)
    pushes = [
        remote(floor_logits, floor_v.at[0], floor_ss, floor_rs, kv, 1),
        remote(round_v.at[0], round_v.at[0], past_ss, past_rs, kv, 1),
        push,
    ]

    @pl.when(tp == 0)
    def _():
        for copy in pushes[:2] + again + pushes[2:]:
            copy.start()

    @pl.when(tp == 1)
    def _():
        pltpu.make_async_copy(w_out, wout_v.at[1], local_sem.at[10]).start()

    c_floor.wait()
    c_hgain.wait()
    square = sq_send[kv]
    arrived(sq_recv.at[most], sq_ss, sq_rs)
    for j in hops:
        square = square + sq_recv[hop(j)]
    row_scale = lax.rsqrt(square / D + epsilon)
    row_scale = jnp.concatenate(
        [jnp.broadcast_to(row_scale[s : s + 1], (H, DK)) for s in range(RL)], axis=0
    )

    def own_part(i):
        return part[i, pl.ds(kv * RL, RL)].reshape(RL * H, DK)

    def both(half):
        pair = pl.ds(2 * half, 2)
        arrived(part_recv.at[0, pair], part_ss, part_rs.at[0, half])
        arrived(part_recv.at[1, pair, most], part_ss, part_rs.at[1, half])

    def summed(u, i, total):
        for j in hops:
            total = total + part_recv[u, i, hop(j)].astype(F32)
        return total * row_scale

    def total_of(u, i):
        own = part_recv[0, i, kv].astype(F32) if u == 0 else own_part(i)
        return summed(u, i, own)

    def forget_of(u, total):
        lower = sigmoid(floor_v[u])
        lower = jnp.concatenate([lower] * RL, axis=0)
        return lower + (1.0 - lower) * sigmoid(total)

    owner = lax.broadcasted_iota(jnp.int32, (RL * H, DK), 0)

    def weighted(u, forget, activ):
        weight = activ * forget
        left = jnp.concatenate(
            [jnp.where(owner == i, weight, 0.0).astype(BF16) for i in range(RL * H)], axis=1
        )
        return (
            jnp.dot(left, round_v[u], preferred_element_type=F32),
            jnp.sum(activ * (1.0 - forget), axis=1, keepdims=True),
        )

    def gated(u, head_out, gate_pre):
        normed = head_out * lax.rsqrt(
            jnp.mean(head_out * head_out, axis=1, keepdims=True) + epsilon
        )
        mix_all[kv, u] = (normed * hgain_v[...] * silu(gate_pre)).astype(BF16)

    @pl.when(tp == 0)
    def _():
        arrived(part_recv.at[0, 0, most], part_ss, part_rs.at[0, 0])
        arrived(part_recv.at[0, 2, most], part_ss, part_rs.at[0, 1])

    @pl.when(tp == 1)
    def _():
        both(0)

    forget = forget_of(tp, summed(tp, 0, own_part(0)))
    mix_sends = [
        remote(mix_all.at[kv], mix_all.at[kv], mix_ss, mix_rs.at[kv], hop(j), 1)
        for j in hops[::-1]
    ]

    @pl.when(tp == 1)
    def _():
        arrived(floor_v.at[0], floor_ss, floor_rs)
        arrived(round_v.at[0], past_ss, past_rs)
        zero, zero_rest = weighted(0, forget_of(0, total_of(0, 0)), silu(total_of(0, 1)))
        one, one_rest = weighted(1, forget, silu(total_of(1, 1)))
        both(1)
        gated(0, zero + total_of(0, 2) * zero_rest, total_of(0, 3))
        gated(1, one + total_of(1, 2) * one_rest, total_of(1, 3))
        for copy in mix_sends:
            copy.start()

    def turn(copy, src, dst):
        copy.wait()
        step = 256 if D % 256 == 0 else D
        for c in range(0, D, step):
            dst[c : c + step, :] = src[:, c : c + step].T

    turn(c_wgate, wgate_v, gatet_v)
    turn(c_wup, wup_v, upt_v)

    def spread(t, k):
        mix_f[t, pl.ds(k * RL, RL)] = mix_all[k, t].astype(F32).reshape(RL, H, DV)

    given = []
    for t in range(T):
        slot = mid_all.at[kv * T + t]
        for j in hops[::-1] + [0]:
            for peer in range(1 if j == 0 else T):
                given.append(
                    remote(slot, slot, mid_ss.at[t], mid_rs.at[kv, t], hop(j), peer)
                )

    @pl.when(tp == 1)
    def _():
        for j in [0] + hops:
            k = hop(j)
            if j:
                arrived(mix_all.at[k], mix_ss, mix_rs.at[k])
            for t in range(T):
                spread(t, k)
        every_head = jnp.concatenate(
            [mix_f[t, :, h, :].astype(BF16) for t in range(T) for h in range(H)], axis=1
        )
        pltpu.make_async_copy(w_out, wout_v.at[1], local_sem.at[10]).wait()
        arrived(wout_v.at[0], wout_ss, wout_rs)
        for t in range(T):
            middle = tok_v[t].astype(F32) + jnp.dot(
                every_head, wout_v[t], preferred_element_type=F32
            )
            mid_all[kv * T + t] = middle.astype(BF16)
            for copy in given[t * len(given) // T : (t + 1) * len(given) // T]:
                copy.start()

    c_mlpg.wait()
    square = jnp.zeros((R, 1), F32)
    gate = None
    if W % 128 == 0:
        groups = [[(j, t)] for j in [0] + hops for t in range(T)]
    else:
        groups = [[(j, t) for t in range(T)] for j in [0] + hops]
    for group in groups:
        k = hop(group[0][0])
        for j, t in group:
            if j:
                arrived(mid_all.at[k * T + t], mid_ss.at[t], mid_rs.at[k, t])
            else:

                @pl.when(tp == 0)
                def _(t=t):
                    arrived(mid_all.at[kv * T + t], mid_ss.at[t], mid_rs.at[kv, t])

        j = k * T + group[0][1]
        blocks = []
        for i in range(len(group)):
            block = mid_all[j + i].astype(F32)
            square = square + jnp.sum(block * block, axis=1, keepdims=True)
            blocks.append((block * mlpg_v[j + i]).astype(BF16))
        block = jnp.concatenate(blocks, axis=1) if len(blocks) > 1 else blocks[0]
        width = len(group) * W
        lanes = pl.ds(pl.multiple_of(j * W, width), width)
        g = jnp.dot(block, gatet_v[lanes, :], preferred_element_type=F32)
        u = jnp.dot(block, upt_v[lanes, :], preferred_element_type=F32)
        gate, upward = (g, u) if gate is None else (gate + g, upward + u)
    mlp_scale = lax.rsqrt(square / D + epsilon)
    hidden = (silu(gate * mlp_scale) * (upward * mlp_scale)).astype(BF16)
    c_wdown.wait()
    for dk in hops[::-1] + [0]:
        k, _ = other(dk, 0)
        lanes = pl.ds(pl.multiple_of(k * T * W, T * W), T * W)
        chunk = jnp.dot(hidden, wdown_v[:, lanes], preferred_element_type=F32).astype(BF16)
        for t in range(T):
            term_send[k * T + t] = chunk[:, t * W : (t + 1) * W]
        for dt in range(0 if dk else 1, T):
            _, t = other(dk, dt)
            send(term_send.at[k * T + t], term_recv.at[me], term_ss, term_rs, k, t)
    value = summed(tp, 2, own_part(2))
    columns = forget.T
    for s in range(RL):
        for h in range(H):
            i = s * H + h
            row = value[i : i + 1, :]
            new_state[s, h] = row + columns[:, i : i + 1] * (past_v[s, h] - row)

    total = term_send[me].astype(F32)
    arrived(term_recv.at[pl.ds(0, K * T - 1)], term_ss, term_rs)
    for dk, dt in near:
        k, t = source(dk, dt)
        total = total + term_recv[k * T + t].astype(F32)
    result[...] = (mid_all[me].astype(F32) + total).astype(BF16)
    swap.wait_send()
    left(sq_send.at[most], sq_ss)
    left(term_send.at[pl.ds(0, K * T - 1)], term_ss)

    @pl.when(tp == 0)
    def _():
        left(part_send, part_ss)
        left(part_send.at[pl.ds(0, 2), most], again_ss)
        for copy in pushes:
            copy.wait_send()

    @pl.when(tp == 1)
    def _():
        left(part_send.at[:, most], part_ss)
        left(mix_all.at[most], mix_ss)
        for t in range(T):
            left(mid_all.at[pl.ds(0, K * T - 1)], mid_ss.at[t])


def flush(result_v, state_v, result, new_state, sem):
    copies = [
        pltpu.make_async_copy(state_v, new_state, sem.at[0]),
        pltpu.make_async_copy(result_v, result, sem.at[1]),
    ]
    for copy in copies:
        copy.start()
    for copy in copies:
        copy.wait()


def body(
    tokens,
    past_state,
    mix_gain,
    w_query,
    w_forget,
    w_value,
    w_gate_out,
    floor_logits,
    head_gain,
    w_out,
    mlp_gain,
    w_gate,
    w_up,
    w_down,
):
    K = lax.axis_size("kv")
    T = lax.axis_size("tp")
    assert T == 2
    n = K * T
    R, W = tokens.shape
    RL, H, DK, DV = past_state.shape
    args = (
        tokens,
        past_state,
        mix_gain.reshape(T, 1, W),
        w_query,
        w_forget,
        w_value,
        w_gate_out,
        floor_logits.reshape(H, DK),
        head_gain.reshape(1, DV),
        w_out,
        mlp_gain.reshape(n, 1, W),
        w_gate.T,
        w_up.T,
        w_down,
    )
    V = pltpu.VMEM
    dma = pltpu.SemaphoreType.DMA
    anywhere = pl.BlockSpec(memory_space=pl.ANY)
    outs = pl.pallas_call(
        functools.partial(kernel, K, T),
        out_shape=(
            pltpu.VMEM((R, W), BF16),
            pltpu.VMEM(past_state.shape, F32),
        ),
        in_specs=[anywhere] * len(args),
        out_specs=(pl.BlockSpec(memory_space=pltpu.VMEM),)*2,
        scratch_shapes=[
            V((T, R, W), BF16),
            V(past_state.shape, F32),
            V((T, 1, W), F32),
            V((4,) + w_query.shape, BF16),
            V((T, H, DK), F32),
            V((1, DV), F32),
            V((T,) + w_out.shape, BF16),
            V((n, 1, W), F32),
            V(w_gate.shape[::-1], BF16),
            V(w_up.shape[::-1], BF16),
            V(w_gate.shape, BF16),
            V(w_up.shape, BF16),
            V(w_down.shape, BF16),
            V((K, RL, DK), F32),
            V((K, RL, DK), F32),
            V((4, R, H, DK), F32),
            V((4, K, RL * H, DK), BF16),
            V((T, 4, K, RL * H, DK), BF16),
            V((T, RL * H * DK, DV), BF16),
            V((K, T, RL * H, DV), BF16),
            V((T, R, H, DV), F32),
            V((n, R, W), BF16),
            V((n, R, W), BF16),
            V((n, R, W), BF16),
            dma((14,)),
            pltpu.SemaphoreType.REGULAR,
            dma,
            dma,
            dma,
            dma,
            dma,
            dma((T, 2)),
            dma,
            dma,
            dma,
            dma,
            dma,
            dma,
            dma,
            dma,
            dma((K,)),
            dma((T,)),
            dma((K, T)),
            dma,
            dma,
        ],
        compiler_params=pltpu.CompilerParams(
            collective_id=0, has_side_effects=True, vmem_limit_bytes=60 * 1024 * 1024
        ),
    )(*args)
    return pl.pallas_call(
        flush,
        out_shape=(
            jax.ShapeDtypeStruct((R, W), BF16),
            jax.ShapeDtypeStruct(past_state.shape, F32),
        ),
        in_specs=[pl.BlockSpec(memory_space=V)] * 2,
        out_specs=(anywhere,) * 2,
        scratch_shapes=[dma((2,))],
        compiler_params=pltpu.CompilerParams(vmem_limit_bytes=1024 * 1024),
    )(*outs)


def solution(mesh):
    placed = (
        P(("grp", "dp"), ("kv", "tp")),
        P(("grp", "dp", "kv"), "tp", None, None),
        P("kv"),
        P("kv", "tp"),
        P("kv", "tp"),
        P("kv", "tp"),
        P("kv", "tp"),
        P("tp"),
        P(),
        P(None, ("kv", "tp")),
        P(),
        P(None, ("kv", "tp")),
        P(None, ("kv", "tp")),
        P(("kv", "tp"), None),
    )
    return jax.shard_map(
        body,
        mesh=mesh,
        in_specs=placed,
        out_specs=(P(("grp", "dp"), ("kv", "tp")), P(("grp", "dp", "kv"), "tp", None, None)),
        check_vma=False,
    )
```

```python
import functools

import jax
import jax.numpy as jnp
from jax import lax
from jax.experimental import pallas as pl
from jax.experimental.pallas import tpu as pltpu
from jax.sharding import PartitionSpec as P

epsilon = 1e-06
F32 = jnp.float32
BF16 = jnp.bfloat16
MESH = pl.DeviceIdType.MESH


def sigmoid(a):
    return 1.0 / (1.0 + jnp.exp(-a))


def silu(a):
    return a / (1.0 + jnp.exp(-a))


def kernel(
    K,
    T,
    tokens,
    past,
    mix_gain,
    w_query,
    w_forget,
    w_value,
    w_gate_out,
    floor_logits,
    head_gain,
    w_out,
    mlp_gain,
    w_gate,
    w_up,
    w_down,
    result,
    new_state,
    tok_v,
    past_v,
    mixg_v,
    proj_v,
    floor_v,
    hgain_v,
    wout_v,
    mlpg_v,
    wgate_v,
    wup_v,
    gatet_v,
    upt_v,
    wdown_v,
    sq_send,
    sq_recv,
    part,
    part_send,
    part_recv,
    round_v,
    mix_all,
    mix_f,
    mid_all,
    term_send,
    term_recv,
    local_sem,
    ready,
    tok_ss,
    tok_rs,
    sq_ss,
    sq_rs,
    part_ss,
    part_rs,
    again_ss,
    floor_ss,
    floor_rs,
    past_ss,
    past_rs,
    wout_ss,
    wout_rs,
    mix_ss,
    mix_rs,
    mid_ss,
    mid_rs,
    term_ss,
    term_rs,
):
    R, W = tokens.shape
    RL, H, DK, DV = past.shape
    D = w_gate.shape[1]
    kv = lax.axis_index("kv")
    tp = lax.axis_index("tp")
    me = kv * T + tp

    hops = list(range(1, K))
    near = [(0, dt) for dt in range(1, T)] + [(j, dt) for j in hops for dt in range(T)]
    upper = (2 * kv) // K
    short = upper * (K - 1 - kv) + (1 - upper) * kv
    ahead = 1 - 2 * upper

    def hop(j):
        if j == 0:
            return kv
        both = jnp.minimum(jnp.maximum(2 * short - j + 1, 0), 1)
        step = both * ((j + 1) // 2) * (2 * (j % 2) - 1) + (1 - both) * (j - short)
        return kv + ahead * step

    def other(j, dt):
        return hop(j), (lax.rem(tp + dt, T) if j == 0 else dt)

    def source(j, dt):
        return hop(j), (lax.rem(tp + T - dt, T) if j == 0 else T - 1 - dt)

    def load(i, src, dst):
        copy = pltpu.make_async_copy(src, dst, local_sem.at[i])
        copy.start()
        return copy

    c_tok = load(0, tokens, tok_v.at[tp])
    c_mixg = load(1, mix_gain, mixg_v)
    c_proj = [
        load(2 + i, w, proj_v.at[i])
        for i, w in enumerate((w_forget, w_query, w_value, w_gate_out))
    ]
    c_past = load(6, past, past_v)
    c_floor = load(7, floor_logits, floor_v.at[tp])
    c_hgain = load(8, head_gain, hgain_v)
    c_mlpg = load(9, mlp_gain, mlpg_v)

    barrier = pltpu.get_barrier_semaphore()

    def signal(k, t):
        pl.semaphore_signal(barrier, inc=1, device_id={"kv": k, "tp": t}, device_id_type=MESH)

    for j in hops[::-1]:
        signal(hop(j), 0)

    @pl.when(tp == 0)
    def _():
        signal(kv, 1)

    @pl.when(tp == 1)
    def _():
        pl.semaphore_wait(barrier, 1)
        pl.semaphore_signal(ready, inc=1, device_id={"kv": kv, "tp": 0}, device_id_type=MESH)

    c_tok.wait()

    def remote(src, dst, ss, rs, k, t):
        return pltpu.make_async_remote_copy(
            src_ref=src,
            dst_ref=dst,
            send_sem=ss,
            recv_sem=rs,
            device_id={"kv": k, "tp": t},
            device_id_type=MESH,
        )

    def send(*args):
        copy = remote(*args)
        copy.start()
        return copy

    def arrived(dst, ss, rs):
        pltpu.make_async_remote_copy(
            src_ref=dst,
            dst_ref=dst,
            send_sem=ss,
            recv_sem=rs,
            device_id={"kv": kv, "tp": lax.rem(tp + 1, T)},
            device_id_type=MESH,
        ).wait_recv()

    def left(src, ss):
        pltpu.make_async_remote_copy(
            src_ref=src,
            dst_ref=src,
            send_sem=ss,
            recv_sem=tok_rs,
            device_id={"kv": kv, "tp": 1 - tp},
            device_id_type=MESH,
        ).wait_send()

    most = pl.ds(0, K - 1)
    swap = pltpu.make_async_remote_copy(
        src_ref=tok_v.at[tp],
        dst_ref=tok_v.at[tp],
        send_sem=tok_ss,
        recv_sem=tok_rs,
        device_id={"kv": kv, "tp": 1 - tp},
        device_id_type=MESH,
    )

    @pl.when(tp == 0)
    def _():
        pl.semaphore_wait(ready, 1)

    swap.start()
    c_mixg.wait()

    def features(t):
        block = tok_v[t].astype(F32)
        square = jnp.sum(block * block, axis=1, keepdims=True)
        rows = pl.ds(pl.multiple_of(t * W, W), W)
        return (block * mixg_v[t]).astype(BF16), rows, square

    def project(part_of, i):
        gained, rows, _ = part_of
        return jnp.dot(gained, proj_v[i, rows, :], preferred_element_type=F32)

    def spread_out(i, total):
        for h in range(H):
            part[i, :, h, :] = total[:, h * DK : (h + 1) * DK]
        for k in range(K):
            part_send[i, k] = part[i, k * RL : (k + 1) * RL].reshape(RL * H, DK).astype(BF16)

    def scatter(*which):
        for j in hops[::-1]:
            k = hop(j)
            for i in which:
                send(
                    part_send.at[i, k],
                    part_recv.at[tp, i, kv],
                    part_ss,
                    part_rs.at[tp, max(i - 1, 0)],
                    k,
                    1,
                )
        for i in which:
            own = remote(
                part_send.at[i, kv],
                part_recv.at[0, i, kv],
                part_ss,
                part_rs.at[0, max(i - 1, 0)],
                kv,
                1,
            )
            pl.when(tp == 0)(own.start)

    again = []
    mine = features(tp)
    early = []
    for i in range(2):
        c_proj[i].wait()
        early.append(project(mine, i))
    swap.wait_recv()
    theirs = features(1 - tp)
    square = jnp.broadcast_to(mine[2] + theirs[2], (R, DK))
    for k in range(K):
        sq_send[k] = square[k * RL : (k + 1) * RL]
    totals = [early[i] + project(theirs, i) for i in range(2)]
    spread_out(0, totals[0])
    spread_out(1, totals[1])

    @pl.when(tp == 0)
    def _():
        pl.semaphore_wait(barrier, (K - 1) * T)
        pl.semaphore_signal(ready, inc=1, device_id={"kv": kv, "tp": 1}, device_id_type=MESH)

    @pl.when(tp == 1)
    def _():
        pl.semaphore_wait(ready, 1)

    for j in hops[::-1]:
        k = hop(j)
        send(sq_send.at[k], sq_recv.at[kv], sq_ss, sq_rs, k, tp)
    scatter(0, 1)
    push = remote(w_out, wout_v.at[0], wout_ss, wout_rs, kv, 1)
    c_wgate = load(0, w_gate, wgate_v)
    c_wup = load(1, w_up, wup_v)
    c_wdown = load(2, w_down, wdown_v)
    totals = []
    for i in range(2, 4):
        c_proj[i].wait()
        totals.append(project(mine, i) + project(theirs, i))
    for i in range(2, 4):
        spread_out(i, totals[i - 2])
        scatter(i)

    for i in (0, 2):
        for j in hops[::-1]:
            k = hop(j)
            again.append(
                remote(
                    part_send.at[i, k],
                    part_recv.at[0, i, kv],
                    again_ss,
                    part_rs.at[0, max(i - 1, 0)],
                    k,
                    0,
                )
            )
    c_past.wait()
    for s in range(RL):
        for h in range(H):
            rows = pl.ds((s * H + h) * DK, DK)
            round_v[tp, rows, :] = past_v[s, h].astype(BF16)
    pushes = [
        remote(floor_logits, floor_v.at[0], floor_ss, floor_rs, kv, 1),
        remote(round_v.at[0], round_v.at[0], past_ss, past_rs, kv, 1),
        push,
    ]

    @pl.when(tp == 0)
    def _():
        for copy in pushes[:2] + again + pushes[2:]:
            copy.start()

    @pl.when(tp == 1)
    def _():
        pltpu.make_async_copy(w_out, wout_v.at[1], local_sem.at[3]).start()

    c_floor.wait()
    c_hgain.wait()
    square = sq_send[kv]
    arrived(sq_recv.at[most], sq_ss, sq_rs)
    for j in hops:
        square = square + sq_recv[hop(j)]
    row_scale = lax.rsqrt(square / D + epsilon)
    row_scale = jnp.concatenate(
        [jnp.broadcast_to(row_scale[s : s + 1], (H, DK)) for s in range(RL)], axis=0
    )

    def own_part(i):
        return part[i, pl.ds(kv * RL, RL)].reshape(RL * H, DK)

    def both(first, count):
        which = pl.ds(first, count)
        group = max(first - 1, 0)
        arrived(part_recv.at[0, which], part_ss, part_rs.at[0, group])
        arrived(part_recv.at[1, which, most], part_ss, part_rs.at[1, group])

    def summed(u, i, total):
        for j in hops:
            total = total + part_recv[u, i, hop(j)].astype(F32)
        return total * row_scale

    def total_of(u, i):
        own = part_recv[0, i, kv].astype(F32) if u == 0 else own_part(i)
        return summed(u, i, own)

    def forget_of(u, total):
        lower = sigmoid(floor_v[u])
        lower = jnp.concatenate([lower] * RL, axis=0)
        return lower + (1.0 - lower) * sigmoid(total)

    owner = lax.broadcasted_iota(jnp.int32, (RL * H, DK), 0)

    def weighted(u, forget, activ):
        weight = activ * forget
        left = jnp.concatenate(
            [jnp.where(owner == i, weight, 0.0).astype(BF16) for i in range(RL * H)], axis=1
        )
        return (
            jnp.dot(left, round_v[u], preferred_element_type=F32),
            jnp.sum(activ * (1.0 - forget), axis=1, keepdims=True),
        )

    def normed(head_out):
        return (
            head_out
            * lax.rsqrt(jnp.mean(head_out * head_out, axis=1, keepdims=True) + epsilon)
            * hgain_v[...]
        )

    @pl.when(tp == 0)
    def _():
        arrived(part_recv.at[0, 0, most], part_ss, part_rs.at[0, 0])
        arrived(part_recv.at[0, 2, most], part_ss, part_rs.at[0, 1])

    @pl.when(tp == 1)
    def _():
        both(0, 2)

    forget = forget_of(tp, summed(tp, 0, own_part(0)))
    mix_sends = [
        remote(mix_all.at[kv], mix_all.at[kv], mix_ss, mix_rs.at[kv], hop(j), 1)
        for j in hops[::-1]
    ]

    @pl.when(tp == 1)
    def _():
        arrived(floor_v.at[0], floor_ss, floor_rs)
        arrived(round_v.at[0], past_ss, past_rs)
        zero, zero_rest = weighted(0, forget_of(0, total_of(0, 0)), silu(total_of(0, 1)))
        one, one_rest = weighted(1, forget, silu(total_of(1, 1)))
        both(2, 1)
        zero = normed(zero + total_of(0, 2) * zero_rest)
        one = normed(one + total_of(1, 2) * one_rest)
        both(3, 1)
        mix_all[kv, 0] = (zero * silu(total_of(0, 3))).astype(BF16)
        mix_all[kv, 1] = (one * silu(total_of(1, 3))).astype(BF16)
        for copy in mix_sends:
            copy.start()

    def turn(copy, src, dst):
        copy.wait()
        step = 256 if D % 256 == 0 else D
        for c in range(0, D, step):
            dst[c : c + step, :] = src[:, c : c + step].T

    turn(c_wgate, wgate_v, gatet_v)
    turn(c_wup, wup_v, upt_v)

    def spread(t, k):
        mix_f[t, pl.ds(k * RL, RL)] = mix_all[k, t].astype(F32).reshape(RL, H, DV)

    given = []
    for t in range(T):
        slot = mid_all.at[kv * T + t]
        for j in hops[::-1] + [0]:
            for peer in range(1 if j == 0 else T):
                given.append(
                    remote(slot, slot, mid_ss.at[t], mid_rs.at[kv, t], hop(j), peer)
                )

    @pl.when(tp == 1)
    def _():
        for j in [0] + hops:
            k = hop(j)
            if j:
                arrived(mix_all.at[k], mix_ss, mix_rs.at[k])
            for t in range(T):
                spread(t, k)
        every_head = jnp.concatenate(
            [mix_f[t, :, h, :].astype(BF16) for t in range(T) for h in range(H)], axis=1
        )
        pltpu.make_async_copy(w_out, wout_v.at[1], local_sem.at[3]).wait()
        arrived(wout_v.at[0], wout_ss, wout_rs)
        middle = [
            tok_v[t].astype(F32)
            + jnp.dot(every_head, wout_v[t], preferred_element_type=F32)
            for t in range(T)
        ]
        for t in range(T):
            mid_all[kv * T + t] = middle[t].astype(BF16)
            for copy in given[t * len(given) // T : (t + 1) * len(given) // T]:
                copy.start()

    c_mlpg.wait()
    square = jnp.zeros((R, 1), F32)
    gate = None
    if W % 128 == 0:
        groups = [[(j, t)] for j in [0] + hops for t in range(T)]
    else:
        groups = [[(j, t) for t in range(T)] for j in [0] + hops]
    for group in groups:
        k = hop(group[0][0])
        for j, t in group:
            if j:
                arrived(mid_all.at[k * T + t], mid_ss.at[t], mid_rs.at[k, t])
            else:

                @pl.when(tp == 0)
                def _(t=t):
                    arrived(mid_all.at[kv * T + t], mid_ss.at[t], mid_rs.at[kv, t])

        j = k * T + group[0][1]
        blocks = []
        for i in range(len(group)):
            block = mid_all[j + i].astype(F32)
            square = square + jnp.sum(block * block, axis=1, keepdims=True)
            blocks.append((block * mlpg_v[j + i]).astype(BF16))
        block = jnp.concatenate(blocks, axis=1) if len(blocks) > 1 else blocks[0]
        width = len(group) * W
        lanes = pl.ds(pl.multiple_of(j * W, width), width)
        g = jnp.dot(block, gatet_v[lanes, :], preferred_element_type=F32)
        u = jnp.dot(block, upt_v[lanes, :], preferred_element_type=F32)
        gate, upward = (g, u) if gate is None else (gate + g, upward + u)
    mlp_scale = lax.rsqrt(square / D + epsilon)
    hidden = (silu(gate * mlp_scale) * (upward * mlp_scale)).astype(BF16)
    c_wdown.wait()
    span = 1 if W % 128 == 0 else T
    last = None

    def give(j, first, chunk):
        for t in range(first, first + span):
            slot = hop(j) * T + t
            term_send[slot] = chunk[:, (t - first) * W : (t - first + 1) * W].astype(BF16)
            copy = remote(term_send.at[slot], term_recv.at[me], term_ss, term_rs, hop(j), t)
            if j:
                copy.start()
            else:
                pl.when(tp != t)(copy.start)

    for j in hops[::-1] + [0]:
        for first in range(0, T, span):
            lanes = pl.ds(pl.multiple_of((hop(j) * T + first) * W, span * W), span * W)
            chunk = jnp.dot(hidden, wdown_v[:, lanes], preferred_element_type=F32)
            if last is not None:
                give(*last)
            last = (j, first, chunk)
    give(*last)
    value = summed(tp, 2, own_part(2))
    columns = forget.T
    for s in range(RL):
        for h in range(H):
            i = s * H + h
            row = value[i : i + 1, :]
            new_state[s, h] = row + columns[:, i : i + 1] * (past_v[s, h] - row)

    total = term_send[me].astype(F32)
    swap.wait_send()
    left(sq_send.at[most], sq_ss)

    @pl.when(tp == 0)
    def _():
        left(part_send, part_ss)
        left(part_send.at[pl.ds(0, 2), most], again_ss)
        for copy in pushes:
            copy.wait_send()

    @pl.when(tp == 1)
    def _():
        left(part_send.at[:, most], part_ss)
        left(mix_all.at[most], mix_ss)
        for t in range(T):
            left(mid_all.at[pl.ds(0, K * T - 1)], mid_ss.at[t])

    arrived(term_recv.at[pl.ds(0, K * T - 1)], term_ss, term_rs)
    for dk, dt in near:
        k, t = source(dk, dt)
        total = total + term_recv[k * T + t].astype(F32)
    result[...] = (mid_all[me].astype(F32) + total).astype(BF16)
    left(term_send.at[pl.ds(0, K * T - 1)], term_ss)


def flush(result_v, state_v, result, new_state, sem):
    copies = [
        pltpu.make_async_copy(state_v, new_state, sem.at[0]),
        pltpu.make_async_copy(result_v, result, sem.at[1]),
    ]
    for copy in copies:
        copy.start()
    for copy in copies:
        copy.wait()


def body(
    tokens,
    past_state,
    mix_gain,
    w_query,
    w_forget,
    w_value,
    w_gate_out,
    floor_logits,
    head_gain,
    w_out,
    mlp_gain,
    w_gate,
    w_up,
    w_down,
):
    K = lax.axis_size("kv")
    T = lax.axis_size("tp")
    assert T == 2
    n = K * T
    R, W = tokens.shape
    RL, H, DK, DV = past_state.shape
    args = (
        tokens,
        past_state,
        mix_gain.reshape(T, 1, W),
        w_query,
        w_forget,
        w_value,
        w_gate_out,
        floor_logits.reshape(H, DK),
        head_gain.reshape(1, DV),
        w_out,
        mlp_gain.reshape(n, 1, W),
        w_gate.T,
        w_up.T,
        w_down,
    )
    V = pltpu.VMEM
    dma = pltpu.SemaphoreType.DMA
    anywhere = pl.BlockSpec(memory_space=pl.ANY)
    outs = pl.pallas_call(
        functools.partial(kernel, K, T),
        out_shape=(
            pltpu.VMEM((R, W), BF16),
            pltpu.VMEM(past_state.shape, F32),
        ),
        in_specs=[anywhere] * len(args),
        out_specs=(pl.BlockSpec(memory_space=pltpu.VMEM),)*2,
        scratch_shapes=[
            V((T, R, W), BF16),
            V(past_state.shape, F32),
            V((T, 1, W), F32),
            V((4,) + w_query.shape, BF16),
            V((T, H, DK), F32),
            V((1, DV), F32),
            V((T,) + w_out.shape, BF16),
            V((n, 1, W), F32),
            V(w_gate.shape[::-1], BF16),
            V(w_up.shape[::-1], BF16),
            V(w_gate.shape, BF16),
            V(w_up.shape, BF16),
            V(w_down.shape, BF16),
            V((K, RL, DK), F32),
            V((K, RL, DK), F32),
            V((4, R, H, DK), F32),
            V((4, K, RL * H, DK), BF16),
            V((T, 4, K, RL * H, DK), BF16),
            V((T, RL * H * DK, DV), BF16),
            V((K, T, RL * H, DV), BF16),
            V((T, R, H, DV), F32),
            V((n, R, W), BF16),
            V((n, R, W), BF16),
            V((n, R, W), BF16),
            dma((10,)),
            pltpu.SemaphoreType.REGULAR,
            dma,
            dma,
            dma,
            dma,
            dma,
            dma((T, 3)),
            dma,
            dma,
            dma,
            dma,
            dma,
            dma,
            dma,
            dma,
            dma((K,)),
            dma((T,)),
            dma((K, T)),
            dma,
            dma,
        ],
        compiler_params=pltpu.CompilerParams(
            collective_id=0, has_side_effects=True, vmem_limit_bytes=60 * 1024 * 1024
        ),
    )(*args)
    return pl.pallas_call(
        flush,
        out_shape=(
            jax.ShapeDtypeStruct((R, W), BF16),
            jax.ShapeDtypeStruct(past_state.shape, F32),
        ),
        in_specs=[pl.BlockSpec(memory_space=V)] * 2,
        out_specs=(anywhere,) * 2,
        scratch_shapes=[dma((2,))],
        compiler_params=pltpu.CompilerParams(vmem_limit_bytes=1024 * 1024),
    )(*outs)


def solution(mesh):
    placed = (
        P(("grp", "dp"), ("kv", "tp")),
        P(("grp", "dp", "kv"), "tp", None, None),
        P("kv"),
        P("kv", "tp"),
        P("kv", "tp"),
        P("kv", "tp"),
        P("kv", "tp"),
        P("tp"),
        P(),
        P(None, ("kv", "tp")),
        P(),
        P(None, ("kv", "tp")),
        P(None, ("kv", "tp")),
        P(("kv", "tp"), None),
    )
    return jax.shard_map(
        body,
        mesh=mesh,
        in_specs=placed,
        out_specs=(P(("grp", "dp"), ("kv", "tp")), P(("grp", "dp", "kv"), "tp", None, None)),
        check_vma=False,
    )
```

```python
import functools

import jax
import jax.numpy as jnp
from jax import lax
from jax.experimental import pallas as pl
from jax.experimental.pallas import tpu as pltpu
from jax.sharding import PartitionSpec as P

epsilon = 1e-06
F32 = jnp.float32
BF16 = jnp.bfloat16
MESH = pl.DeviceIdType.MESH


def sigmoid(a):
    return 1.0 / (1.0 + jnp.exp(-a))


def silu(a):
    return a / (1.0 + jnp.exp(-a))


def kernel(
    K,
    T,
    tokens,
    past,
    mix_gain,
    w_query,
    w_forget,
    w_value,
    w_gate_out,
    floor_logits,
    head_gain,
    w_out,
    mlp_gain,
    w_gate,
    w_up,
    w_down,
    result,
    new_state,
    tok_v,
    past_v,
    mixg_v,
    proj_v,
    floor_v,
    hgain_v,
    wout_v,
    mlpg_v,
    wgate_v,
    wup_v,
    gatet_v,
    upt_v,
    wdown_v,
    sq_send,
    sq_recv,
    part,
    part_send,
    part_recv,
    round_v,
    mix_all,
    mix_f,
    mid_all,
    term_send,
    term_recv,
    local_sem,
    ready,
    tok_ss,
    tok_rs,
    sq_ss,
    sq_rs,
    part_ss,
    part_rs,
    again_ss,
    floor_ss,
    floor_rs,
    past_ss,
    past_rs,
    wout_ss,
    wout_rs,
    mix_ss,
    mix_rs,
    mid_ss,
    mid_rs,
    term_ss,
    term_rs,
):
    R, W = tokens.shape
    RL, H, DK, DV = past.shape
    D = w_gate.shape[1]
    kv = lax.axis_index("kv")
    tp = lax.axis_index("tp")
    me = kv * T + tp

    hops = list(range(1, K))
    near = [(0, dt) for dt in range(1, T)] + [(j, dt) for j in hops for dt in range(T)]
    upper = (2 * kv) // K
    short = upper * (K - 1 - kv) + (1 - upper) * kv
    ahead = 1 - 2 * upper

    def hop(j):
        if j == 0:
            return kv
        both = jnp.minimum(jnp.maximum(2 * short - j + 1, 0), 1)
        step = both * ((j + 1) // 2) * (2 * (j % 2) - 1) + (1 - both) * (j - short)
        return kv + ahead * step

    def other(j, dt):
        return hop(j), (lax.rem(tp + dt, T) if j == 0 else dt)

    def source(j, dt):
        return hop(j), (lax.rem(tp + T - dt, T) if j == 0 else T - 1 - dt)

    def load(i, src, dst):
        copy = pltpu.make_async_copy(src, dst, local_sem.at[i])
        copy.start()
        return copy

    c_tok = load(0, tokens, tok_v.at[tp])
    c_mixg = load(1, mix_gain, mixg_v)
    c_proj = [
        load(2 + i, w, proj_v.at[i])
        for i, w in enumerate((w_forget, w_query, w_value, w_gate_out))
    ]
    c_past = load(6, past, past_v)
    c_floor = load(7, floor_logits, floor_v.at[tp])
    c_hgain = load(8, head_gain, hgain_v)
    c_mlpg = load(9, mlp_gain, mlpg_v)

    barrier = pltpu.get_barrier_semaphore()

    def signal(k, t):
        pl.semaphore_signal(barrier, inc=1, device_id={"kv": k, "tp": t}, device_id_type=MESH)

    for j in hops[::-1]:
        signal(hop(j), 0)

    @pl.when(tp == 0)
    def _():
        signal(kv, 1)

    @pl.when(tp == 1)
    def _():
        pl.semaphore_wait(barrier, 1)
        pl.semaphore_signal(ready, inc=1, device_id={"kv": kv, "tp": 0}, device_id_type=MESH)

    c_tok.wait()

    def remote(src, dst, ss, rs, k, t):
        return pltpu.make_async_remote_copy(
            src_ref=src,
            dst_ref=dst,
            send_sem=ss,
            recv_sem=rs,
            device_id={"kv": k, "tp": t},
            device_id_type=MESH,
        )

    def send(*args):
        copy = remote(*args)
        copy.start()
        return copy

    def arrived(dst, ss, rs):
        pltpu.make_async_remote_copy(
            src_ref=dst,
            dst_ref=dst,
            send_sem=ss,
            recv_sem=rs,
            device_id={"kv": kv, "tp": lax.rem(tp + 1, T)},
            device_id_type=MESH,
        ).wait_recv()

    def left(src, ss):
        pltpu.make_async_remote_copy(
            src_ref=src,
            dst_ref=src,
            send_sem=ss,
            recv_sem=tok_rs,
            device_id={"kv": kv, "tp": 1 - tp},
            device_id_type=MESH,
        ).wait_send()

    most = pl.ds(0, K - 1)
    swap = pltpu.make_async_remote_copy(
        src_ref=tok_v.at[tp],
        dst_ref=tok_v.at[tp],
        send_sem=tok_ss,
        recv_sem=tok_rs,
        device_id={"kv": kv, "tp": 1 - tp},
        device_id_type=MESH,
    )

    @pl.when(tp == 0)
    def _():
        pl.semaphore_wait(ready, 1)

    swap.start()
    c_mixg.wait()

    def features(t):
        block = tok_v[t].astype(F32)
        square = jnp.sum(block * block, axis=1, keepdims=True)
        rows = pl.ds(pl.multiple_of(t * W, W), W)
        return (block * mixg_v[t]).astype(BF16), rows, square

    def project(part_of, i):
        gained, rows, _ = part_of
        return jnp.dot(gained, proj_v[i, rows, :], preferred_element_type=F32)

    def spread_out(i, total):
        for h in range(H):
            part[i, :, h, :] = total[:, h * DK : (h + 1) * DK]
        for k in range(K):
            part_send[i, k] = part[i, k * RL : (k + 1) * RL].reshape(RL * H, DK).astype(BF16)

    def scatter(*which):
        for j in hops[::-1]:
            k = hop(j)
            for i in which:
                send(
                    part_send.at[i, k],
                    part_recv.at[tp, i, kv],
                    part_ss,
                    part_rs.at[tp, max(i - 1, 0)],
                    k,
                    1,
                )
        for i in which:
            own = remote(
                part_send.at[i, kv],
                part_recv.at[0, i, kv],
                part_ss,
                part_rs.at[0, max(i - 1, 0)],
                kv,
                1,
            )
            pl.when(tp == 0)(own.start)

    again = []
    mine = features(tp)
    early = []
    for i in range(2):
        c_proj[i].wait()
        early.append(project(mine, i))
    swap.wait_recv()
    theirs = features(1 - tp)
    square = jnp.broadcast_to(mine[2] + theirs[2], (R, DK))
    for k in range(K):
        sq_send[k] = square[k * RL : (k + 1) * RL]
    totals = [early[i] + project(theirs, i) for i in range(2)]
    spread_out(0, totals[0])
    spread_out(1, totals[1])

    @pl.when(tp == 0)
    def _():
        pl.semaphore_wait(barrier, (K - 1) * T)
        pl.semaphore_signal(ready, inc=1, device_id={"kv": kv, "tp": 1}, device_id_type=MESH)

    @pl.when(tp == 1)
    def _():
        pl.semaphore_wait(ready, 1)

    for j in hops[::-1]:
        k = hop(j)
        send(sq_send.at[k], sq_recv.at[kv], sq_ss, sq_rs, k, tp)
    scatter(0, 1)
    push = remote(w_out, wout_v.at[0], wout_ss, wout_rs, kv, 1)
    c_wgate = load(0, w_gate, wgate_v)
    c_wup = load(1, w_up, wup_v)
    c_wdown = load(2, w_down, wdown_v)
    totals = []
    for i in range(2, 4):
        c_proj[i].wait()
        totals.append(project(mine, i) + project(theirs, i))
    for i in range(2, 4):
        spread_out(i, totals[i - 2])
        scatter(i)

    for i in (0, 2):
        for j in hops[::-1]:
            k = hop(j)
            again.append(
                remote(
                    part_send.at[i, k],
                    part_recv.at[0, i, kv],
                    again_ss,
                    part_rs.at[0, max(i - 1, 0)],
                    k,
                    0,
                )
            )
    c_past.wait()
    for s in range(RL):
        for h in range(H):
            rows = pl.ds((s * H + h) * DK, DK)
            round_v[tp, rows, :] = past_v[s, h].astype(BF16)
    pushes = [
        remote(floor_logits, floor_v.at[0], floor_ss, floor_rs, kv, 1),
        remote(round_v.at[0], round_v.at[0], past_ss, past_rs, kv, 1),
        push,
    ]

    @pl.when(tp == 0)
    def _():
        for copy in pushes[:2] + again + pushes[2:]:
            copy.start()

    @pl.when(tp == 1)
    def _():
        pltpu.make_async_copy(w_out, wout_v.at[1], local_sem.at[3]).start()

    c_floor.wait()
    c_hgain.wait()
    square = sq_send[kv]
    arrived(sq_recv.at[most], sq_ss, sq_rs)
    for j in hops:
        square = square + sq_recv[hop(j)]
    row_scale = lax.rsqrt(square / D + epsilon)
    row_scale = jnp.concatenate(
        [jnp.broadcast_to(row_scale[s : s + 1], (H, DK)) for s in range(RL)], axis=0
    )

    def own_part(i):
        return part[i, pl.ds(kv * RL, RL)].reshape(RL * H, DK)

    def both(first, count):
        which = pl.ds(first, count)
        group = max(first - 1, 0)
        arrived(part_recv.at[0, which], part_ss, part_rs.at[0, group])
        arrived(part_recv.at[1, which, most], part_ss, part_rs.at[1, group])

    def summed(u, i, total):
        for j in hops:
            total = total + part_recv[u, i, hop(j)].astype(F32)
        return total * row_scale

    def total_of(u, i):
        own = part_recv[0, i, kv].astype(F32) if u == 0 else own_part(i)
        return summed(u, i, own)

    def forget_of(u, total):
        lower = sigmoid(floor_v[u])
        lower = jnp.concatenate([lower] * RL, axis=0)
        return lower + (1.0 - lower) * sigmoid(total)

    owner = lax.broadcasted_iota(jnp.int32, (RL * H, DK), 0)

    def weighted(u, forget, activ):
        weight = activ * forget
        left = jnp.concatenate(
            [jnp.where(owner == i, weight, 0.0).astype(BF16) for i in range(RL * H)], axis=1
        )
        return (
            halves(left, round_v.at[u]),
            jnp.sum(activ * (1.0 - forget), axis=1, keepdims=True),
        )

    def halves(a, b):
        cut = b.shape[0] // 2
        first = jnp.dot(a[:, :cut], b[:cut, :], preferred_element_type=F32)
        return first + jnp.dot(a[:, cut:], b[cut:, :], preferred_element_type=F32)

    def normed(head_out):
        return (
            head_out
            * lax.rsqrt(jnp.mean(head_out * head_out, axis=1, keepdims=True) + epsilon)
            * hgain_v[...]
        )

    @pl.when(tp == 0)
    def _():
        arrived(part_recv.at[0, 0, most], part_ss, part_rs.at[0, 0])
        arrived(part_recv.at[0, 2, most], part_ss, part_rs.at[0, 1])

    @pl.when(tp == 1)
    def _():
        both(0, 2)

    forget = forget_of(tp, summed(tp, 0, own_part(0)))
    mix_sends = [
        remote(mix_all.at[kv], mix_all.at[kv], mix_ss, mix_rs.at[kv], hop(j), 1)
        for j in hops[::-1]
    ]

    @pl.when(tp == 1)
    def _():
        arrived(floor_v.at[0], floor_ss, floor_rs)
        arrived(round_v.at[0], past_ss, past_rs)
        zero, zero_rest = weighted(0, forget_of(0, total_of(0, 0)), silu(total_of(0, 1)))
        one, one_rest = weighted(1, forget, silu(total_of(1, 1)))
        both(2, 1)
        zero = normed(zero + total_of(0, 2) * zero_rest)
        one = normed(one + total_of(1, 2) * one_rest)
        both(3, 1)
        mix_all[kv, 0] = (zero * silu(total_of(0, 3))).astype(BF16)
        mix_all[kv, 1] = (one * silu(total_of(1, 3))).astype(BF16)
        for copy in mix_sends:
            copy.start()

    def turn(copy, src, dst):
        copy.wait()
        step = 256 if D % 256 == 0 else D
        for c in range(0, D, step):
            dst[c : c + step, :] = src[:, c : c + step].T

    turn(c_wgate, wgate_v, gatet_v)
    turn(c_wup, wup_v, upt_v)

    def spread(t, k):
        mix_f[t, pl.ds(k * RL, RL)] = mix_all[k, t].astype(F32).reshape(RL, H, DV)

    given = []
    for t in range(T):
        slot = mid_all.at[kv * T + t]
        for j in hops[::-1] + [0]:
            for peer in range(1 if j == 0 else T):
                given.append(
                    remote(slot, slot, mid_ss.at[t], mid_rs.at[kv, t], hop(j), peer)
                )

    @pl.when(tp == 1)
    def _():
        for j in [0] + hops:
            k = hop(j)
            if j:
                arrived(mix_all.at[k], mix_ss, mix_rs.at[k])
            for t in range(T):
                spread(t, k)
        every_head = jnp.concatenate(
            [mix_f[t, :, h, :].astype(BF16) for t in range(T) for h in range(H)], axis=1
        )
        pltpu.make_async_copy(w_out, wout_v.at[1], local_sem.at[3]).wait()
        arrived(wout_v.at[0], wout_ss, wout_rs)
        middle = [
            tok_v[t].astype(F32)
            + halves(every_head, wout_v.at[t])
            for t in range(T)
        ]
        for t in range(T):
            mid_all[kv * T + t] = middle[t].astype(BF16)
            for copy in given[t * len(given) // T : (t + 1) * len(given) // T]:
                copy.start()

    c_mlpg.wait()
    square = jnp.zeros((R, 1), F32)
    gate = None
    if W % 128 == 0:
        groups = [[(j, t)] for j in [0] + hops for t in range(T)]
    else:
        groups = [[(j, t) for t in range(T)] for j in [0] + hops]
    for group in groups:
        k = hop(group[0][0])
        for j, t in group:
            if j:
                arrived(mid_all.at[k * T + t], mid_ss.at[t], mid_rs.at[k, t])
            else:

                @pl.when(tp == 0)
                def _(t=t):
                    arrived(mid_all.at[kv * T + t], mid_ss.at[t], mid_rs.at[kv, t])

        j = k * T + group[0][1]
        blocks = []
        for i in range(len(group)):
            block = mid_all[j + i].astype(F32)
            square = square + jnp.sum(block * block, axis=1, keepdims=True)
            blocks.append((block * mlpg_v[j + i]).astype(BF16))
        block = jnp.concatenate(blocks, axis=1) if len(blocks) > 1 else blocks[0]
        width = len(group) * W
        lanes = pl.ds(pl.multiple_of(j * W, width), width)
        g = jnp.dot(block, gatet_v[lanes, :], preferred_element_type=F32)
        u = jnp.dot(block, upt_v[lanes, :], preferred_element_type=F32)
        gate, upward = (g, u) if gate is None else (gate + g, upward + u)
    mlp_scale = lax.rsqrt(square / D + epsilon)
    hidden = (silu(gate * mlp_scale) * (upward * mlp_scale)).astype(BF16)
    c_wdown.wait()
    span = 1 if W % 128 == 0 else T
    last = None

    def give(j, first, chunk):
        for t in range(first, first + span):
            slot = hop(j) * T + t
            term_send[slot] = chunk[:, (t - first) * W : (t - first + 1) * W].astype(BF16)
            copy = remote(term_send.at[slot], term_recv.at[me], term_ss, term_rs, hop(j), t)
            if j:
                copy.start()
            else:
                pl.when(tp != t)(copy.start)

    for j in hops[::-1] + [0]:
        for first in range(0, T, span):
            lanes = pl.ds(pl.multiple_of((hop(j) * T + first) * W, span * W), span * W)
            chunk = jnp.dot(hidden, wdown_v[:, lanes], preferred_element_type=F32)
            if last is not None:
                give(*last)
            last = (j, first, chunk)
    give(*last)
    value = summed(tp, 2, own_part(2))
    columns = forget.T
    for s in range(RL):
        for h in range(H):
            i = s * H + h
            row = value[i : i + 1, :]
            new_state[s, h] = row + columns[:, i : i + 1] * (past_v[s, h] - row)

    total = term_send[me].astype(F32)
    swap.wait_send()
    left(sq_send.at[most], sq_ss)

    @pl.when(tp == 0)
    def _():
        left(part_send, part_ss)
        left(part_send.at[pl.ds(0, 2), most], again_ss)
        for copy in pushes:
            copy.wait_send()

    @pl.when(tp == 1)
    def _():
        left(part_send.at[:, most], part_ss)
        left(mix_all.at[most], mix_ss)
        for t in range(T):
            left(mid_all.at[pl.ds(0, K * T - 1)], mid_ss.at[t])

    arrived(term_recv.at[pl.ds(0, K * T - 1)], term_ss, term_rs)
    for dk, dt in near:
        k, t = source(dk, dt)
        total = total + term_recv[k * T + t].astype(F32)
    result[...] = (mid_all[me].astype(F32) + total).astype(BF16)
    left(term_send.at[pl.ds(0, K * T - 1)], term_ss)


def flush(result_v, state_v, result, new_state, sem):
    copies = [
        pltpu.make_async_copy(state_v, new_state, sem.at[0]),
        pltpu.make_async_copy(result_v, result, sem.at[1]),
    ]
    for copy in copies:
        copy.start()
    for copy in copies:
        copy.wait()


def body(
    tokens,
    past_state,
    mix_gain,
    w_query,
    w_forget,
    w_value,
    w_gate_out,
    floor_logits,
    head_gain,
    w_out,
    mlp_gain,
    w_gate,
    w_up,
    w_down,
):
    K = lax.axis_size("kv")
    T = lax.axis_size("tp")
    assert T == 2
    n = K * T
    R, W = tokens.shape
    RL, H, DK, DV = past_state.shape
    args = (
        tokens,
        past_state,
        mix_gain.reshape(T, 1, W),
        w_query,
        w_forget,
        w_value,
        w_gate_out,
        floor_logits.reshape(H, DK),
        head_gain.reshape(1, DV),
        w_out,
        mlp_gain.reshape(n, 1, W),
        w_gate.T,
        w_up.T,
        w_down,
    )
    V = pltpu.VMEM
    dma = pltpu.SemaphoreType.DMA
    anywhere = pl.BlockSpec(memory_space=pl.ANY)
    outs = pl.pallas_call(
        functools.partial(kernel, K, T),
        out_shape=(
            pltpu.VMEM((R, W), BF16),
            pltpu.VMEM(past_state.shape, F32),
        ),
        in_specs=[anywhere] * len(args),
        out_specs=(pl.BlockSpec(memory_space=pltpu.VMEM),)*2,
        scratch_shapes=[
            V((T, R, W), BF16),
            V(past_state.shape, F32),
            V((T, 1, W), F32),
            V((4,) + w_query.shape, BF16),
            V((T, H, DK), F32),
            V((1, DV), F32),
            V((T,) + w_out.shape, BF16),
            V((n, 1, W), F32),
            V(w_gate.shape[::-1], BF16),
            V(w_up.shape[::-1], BF16),
            V(w_gate.shape, BF16),
            V(w_up.shape, BF16),
            V(w_down.shape, BF16),
            V((K, RL, DK), F32),
            V((K, RL, DK), F32),
            V((4, R, H, DK), F32),
            V((4, K, RL * H, DK), BF16),
            V((T, 4, K, RL * H, DK), BF16),
            V((T, RL * H * DK, DV), BF16),
            V((K, T, RL * H, DV), BF16),
            V((T, R, H, DV), F32),
            V((n, R, W), BF16),
            V((n, R, W), BF16),
            V((n, R, W), BF16),
            dma((10,)),
            pltpu.SemaphoreType.REGULAR,
            dma,
            dma,
            dma,
            dma,
            dma,
            dma((T, 3)),
            dma,
            dma,
            dma,
            dma,
            dma,
            dma,
            dma,
            dma,
            dma((K,)),
            dma((T,)),
            dma((K, T)),
            dma,
            dma,
        ],
        compiler_params=pltpu.CompilerParams(
            collective_id=0, has_side_effects=True, vmem_limit_bytes=60 * 1024 * 1024
        ),
    )(*args)
    return pl.pallas_call(
        flush,
        out_shape=(
            jax.ShapeDtypeStruct((R, W), BF16),
            jax.ShapeDtypeStruct(past_state.shape, F32),
        ),
        in_specs=[pl.BlockSpec(memory_space=V)] * 2,
        out_specs=(anywhere,) * 2,
        scratch_shapes=[dma((2,))],
        compiler_params=pltpu.CompilerParams(vmem_limit_bytes=1024 * 1024),
    )(*outs)


def solution(mesh):
    placed = (
        P(("grp", "dp"), ("kv", "tp")),
        P(("grp", "dp", "kv"), "tp", None, None),
        P("kv"),
        P("kv", "tp"),
        P("kv", "tp"),
        P("kv", "tp"),
        P("kv", "tp"),
        P("tp"),
        P(),
        P(None, ("kv", "tp")),
        P(),
        P(None, ("kv", "tp")),
        P(None, ("kv", "tp")),
        P(("kv", "tp"), None),
    )
    return jax.shard_map(
        body,
        mesh=mesh,
        in_specs=placed,
        out_specs=(P(("grp", "dp"), ("kv", "tp")), P(("grp", "dp", "kv"), "tp", None, None)),
        check_vma=False,
    )
```

```python
import functools

import jax
import jax.numpy as jnp
from jax import lax
from jax.experimental import pallas as pl
from jax.experimental.pallas import tpu as pltpu
from jax.sharding import PartitionSpec as P

epsilon = 1e-06
F32 = jnp.float32
BF16 = jnp.bfloat16
MESH = pl.DeviceIdType.MESH


def sigmoid(a):
    return 1.0 / (1.0 + jnp.exp(-a))


def silu(a):
    return a / (1.0 + jnp.exp(-a))


def kernel(
    K,
    T,
    tokens,
    past,
    mix_gain,
    w_query,
    w_forget,
    w_value,
    w_gate_out,
    floor_logits,
    head_gain,
    w_out,
    mlp_gain,
    w_gate,
    w_up,
    w_down,
    result,
    new_state,
    tok_v,
    past_v,
    mixg_v,
    proj_v,
    floor_v,
    hgain_v,
    wout_v,
    mlpg_v,
    wgate_v,
    wup_v,
    gatet_v,
    upt_v,
    wdown_v,
    sq_send,
    sq_recv,
    part,
    part_send,
    part_recv,
    round_v,
    mix_all,
    mix_f,
    mid_all,
    term_send,
    term_recv,
    local_sem,
    ready,
    tok_ss,
    tok_rs,
    sq_ss,
    sq_rs,
    part_ss,
    part_rs,
    again_ss,
    floor_ss,
    floor_rs,
    past_ss,
    past_rs,
    wout_ss,
    wout_rs,
    mix_ss,
    mix_rs,
    mid_rs,
    term_rs,
):
    R, W = tokens.shape
    RL, H, DK, DV = past.shape
    D = w_gate.shape[1]
    kv = lax.axis_index("kv")
    tp = lax.axis_index("tp")
    me = kv * T + tp

    hops = list(range(1, K))
    near = [(0, dt) for dt in range(1, T)] + [(j, dt) for j in hops for dt in range(T)]
    upper = (2 * kv) // K
    short = upper * (K - 1 - kv) + (1 - upper) * kv
    ahead = 1 - 2 * upper

    def hop(j):
        if j == 0:
            return kv
        both = jnp.minimum(jnp.maximum(2 * short - j + 1, 0), 1)
        step = both * ((j + 1) // 2) * (2 * (j % 2) - 1) + (1 - both) * (j - short)
        return kv + ahead * step

    def other(j, dt):
        return hop(j), (lax.rem(tp + dt, T) if j == 0 else dt)

    def source(j, dt):
        return hop(j), (lax.rem(tp + T - dt, T) if j == 0 else T - 1 - dt)

    def load(i, src, dst):
        copy = pltpu.make_async_copy(src, dst, local_sem.at[i])
        copy.start()
        return copy

    c_tok = load(0, tokens, tok_v.at[tp])
    c_mixg = load(1, mix_gain, mixg_v)
    c_proj = [
        load(2 + i, w, proj_v.at[i])
        for i, w in enumerate((w_forget, w_query, w_value, w_gate_out))
    ]
    c_past = load(6, past, past_v)
    c_floor = load(7, floor_logits, floor_v.at[tp])
    c_hgain = load(8, head_gain, hgain_v)
    c_mlpg = load(9, mlp_gain, mlpg_v)

    barrier = pltpu.get_barrier_semaphore()

    def signal(k, t):
        pl.semaphore_signal(barrier, inc=1, device_id={"kv": k, "tp": t}, device_id_type=MESH)

    for j in hops[::-1]:
        signal(hop(j), 0)

    @pl.when(tp == 0)
    def _():
        signal(kv, 1)

    @pl.when(tp == 1)
    def _():
        pl.semaphore_wait(barrier, 1)
        pl.semaphore_signal(ready, inc=1, device_id={"kv": kv, "tp": 0}, device_id_type=MESH)

    c_tok.wait()

    def remote(src, dst, ss, rs, k, t):
        return pltpu.make_async_remote_copy(
            src_ref=src,
            dst_ref=dst,
            send_sem=ss,
            recv_sem=rs,
            device_id={"kv": k, "tp": t},
            device_id_type=MESH,
        )

    def send(*args):
        copy = remote(*args)
        copy.start()
        return copy

    def arrived(dst, ss, rs):
        pltpu.make_async_remote_copy(
            src_ref=dst,
            dst_ref=dst,
            send_sem=ss,
            recv_sem=rs,
            device_id={"kv": kv, "tp": lax.rem(tp + 1, T)},
            device_id_type=MESH,
        ).wait_recv()

    def left(src, ss):
        pltpu.make_async_remote_copy(
            src_ref=src,
            dst_ref=src,
            send_sem=ss,
            recv_sem=tok_rs,
            device_id={"kv": kv, "tp": 1 - tp},
            device_id_type=MESH,
        ).wait_send()

    most = pl.ds(0, K - 1)
    swap = pltpu.make_async_remote_copy(
        src_ref=tok_v.at[tp],
        dst_ref=tok_v.at[tp],
        send_sem=tok_ss,
        recv_sem=tok_rs,
        device_id={"kv": kv, "tp": 1 - tp},
        device_id_type=MESH,
    )

    @pl.when(tp == 0)
    def _():
        pl.semaphore_wait(ready, 1)

    swap.start()
    c_mixg.wait()

    def features(t):
        block = tok_v[t].astype(F32)
        square = jnp.sum(block * block, axis=1, keepdims=True)
        rows = pl.ds(pl.multiple_of(t * W, W), W)
        return (block * mixg_v[t]).astype(BF16), rows, square

    def project(part_of, i):
        gained, rows, _ = part_of
        return jnp.dot(gained, proj_v[i, rows, :], preferred_element_type=F32)

    def spread_out(i, total):
        for h in range(H):
            part[i, :, h, :] = total[:, h * DK : (h + 1) * DK]
        for k in range(K):
            part_send[i, k] = part[i, k * RL : (k + 1) * RL].reshape(RL * H, DK).astype(BF16)

    def scatter(*which):
        for j in hops[::-1]:
            k = hop(j)
            for i in which:
                send(
                    part_send.at[i, k],
                    part_recv.at[tp, i, kv],
                    part_ss,
                    part_rs.at[tp, max(i - 1, 0)],
                    k,
                    1,
                )
        for i in which:
            own = remote(
                part_send.at[i, kv],
                part_recv.at[0, i, kv],
                part_ss,
                part_rs.at[0, max(i - 1, 0)],
                kv,
                1,
            )
            pl.when(tp == 0)(own.start)

    again = []
    mine = features(tp)
    early = []
    for i in range(2):
        c_proj[i].wait()
        early.append(project(mine, i))
    swap.wait_recv()
    theirs = features(1 - tp)
    square = jnp.broadcast_to(mine[2] + theirs[2], (R, DK))
    for k in range(K):
        sq_send[k] = square[k * RL : (k + 1) * RL]
    totals = [early[i] + project(theirs, i) for i in range(2)]
    spread_out(0, totals[0])
    spread_out(1, totals[1])

    @pl.when(tp == 0)
    def _():
        pl.semaphore_wait(barrier, (K - 1) * T)
        pl.semaphore_signal(ready, inc=1, device_id={"kv": kv, "tp": 1}, device_id_type=MESH)

    @pl.when(tp == 1)
    def _():
        pl.semaphore_wait(ready, 1)

    for j in hops[::-1]:
        k = hop(j)
        send(sq_send.at[k], sq_recv.at[kv], sq_ss, sq_rs, k, tp)
    scatter(0, 1)
    push = remote(w_out, wout_v.at[0], wout_ss, wout_rs, kv, 1)
    c_wgate = load(0, w_gate, wgate_v)
    c_wup = load(1, w_up, wup_v)
    c_wdown = load(2, w_down, wdown_v)
    totals = []
    for i in range(2, 4):
        c_proj[i].wait()
        totals.append(project(mine, i) + project(theirs, i))
    for i in range(2, 4):
        spread_out(i, totals[i - 2])
        scatter(i)

    for i in (0, 2):
        for j in hops[::-1]:
            k = hop(j)
            again.append(
                remote(
                    part_send.at[i, k],
                    part_recv.at[0, i, kv],
                    again_ss,
                    part_rs.at[0, max(i - 1, 0)],
                    k,
                    0,
                )
            )
    c_past.wait()
    for s in range(RL):
        for h in range(H):
            rows = pl.ds((s * H + h) * DK, DK)
            round_v[tp, rows, :] = past_v[s, h].astype(BF16)
    pushes = [
        remote(floor_logits, floor_v.at[0], floor_ss, floor_rs, kv, 1),
        remote(round_v.at[0], round_v.at[0], past_ss, past_rs, kv, 1),
        push,
    ]

    @pl.when(tp == 0)
    def _():
        for copy in pushes[:2] + again + pushes[2:]:
            copy.start()

    @pl.when(tp == 1)
    def _():
        pltpu.make_async_copy(w_out, wout_v.at[1], local_sem.at[3]).start()

    c_floor.wait()
    c_hgain.wait()
    square = sq_send[kv]
    arrived(sq_recv.at[most], sq_ss, sq_rs)
    for j in hops:
        square = square + sq_recv[hop(j)]
    row_scale = lax.rsqrt(square / D + epsilon)
    row_scale = jnp.concatenate(
        [jnp.broadcast_to(row_scale[s : s + 1], (H, DK)) for s in range(RL)], axis=0
    )

    def own_part(i):
        return part[i, pl.ds(kv * RL, RL)].reshape(RL * H, DK)

    def both(first, count):
        which = pl.ds(first, count)
        group = max(first - 1, 0)
        arrived(part_recv.at[0, which], part_ss, part_rs.at[0, group])
        arrived(part_recv.at[1, which, most], part_ss, part_rs.at[1, group])

    def summed(u, i, total):
        for j in hops:
            total = total + part_recv[u, i, hop(j)].astype(F32)
        return total * row_scale

    def total_of(u, i):
        own = part_recv[0, i, kv].astype(F32) if u == 0 else own_part(i)
        return summed(u, i, own)

    def forget_of(u, total):
        lower = sigmoid(floor_v[u])
        lower = jnp.concatenate([lower] * RL, axis=0)
        return lower + (1.0 - lower) * sigmoid(total)

    owner = lax.broadcasted_iota(jnp.int32, (RL * H, DK), 0)

    def weighted(u, forget, activ):
        weight = activ * forget
        left = jnp.concatenate(
            [jnp.where(owner == i, weight, 0.0).astype(BF16) for i in range(RL * H)], axis=1
        )
        return (
            halves(left, round_v.at[u]),
            jnp.sum(activ * (1.0 - forget), axis=1, keepdims=True),
        )

    def halves(a, b):
        cut = b.shape[0] // 2
        first = jnp.dot(a[:, :cut], b[:cut, :], preferred_element_type=F32)
        return first + jnp.dot(a[:, cut:], b[cut:, :], preferred_element_type=F32)

    def normed(head_out):
        return (
            head_out
            * lax.rsqrt(jnp.mean(head_out * head_out, axis=1, keepdims=True) + epsilon)
            * hgain_v[...]
        )

    @pl.when(tp == 0)
    def _():
        arrived(part_recv.at[0, 0, most], part_ss, part_rs.at[0, 0])
        arrived(part_recv.at[0, 2, most], part_ss, part_rs.at[0, 1])

    @pl.when(tp == 1)
    def _():
        both(0, 2)

    forget = forget_of(tp, summed(tp, 0, own_part(0)))
    mix_sends = [
        remote(mix_all.at[kv], mix_all.at[kv], mix_ss, mix_rs.at[kv], hop(j), 1)
        for j in hops[::-1]
    ]

    @pl.when(tp == 1)
    def _():
        arrived(floor_v.at[0], floor_ss, floor_rs)
        arrived(round_v.at[0], past_ss, past_rs)
        zero, zero_rest = weighted(0, forget_of(0, total_of(0, 0)), silu(total_of(0, 1)))
        one, one_rest = weighted(1, forget, silu(total_of(1, 1)))
        both(2, 1)
        zero = normed(zero + total_of(0, 2) * zero_rest)
        one = normed(one + total_of(1, 2) * one_rest)
        both(3, 1)
        mix_all[kv, 0] = (zero * silu(total_of(0, 3))).astype(BF16)
        mix_all[kv, 1] = (one * silu(total_of(1, 3))).astype(BF16)
        for copy in mix_sends:
            copy.start()

    def turn(copy, src, dst):
        copy.wait()
        step = 256 if D % 256 == 0 else D
        for c in range(0, D, step):
            dst[c : c + step, :] = src[:, c : c + step].T

    swap.wait_send()
    left(sq_send.at[most], sq_ss)

    @pl.when(tp == 0)
    def _():
        left(part_send, part_ss)

    @pl.when(tp == 1)
    def _():
        left(part_send.at[:, most], part_ss)

    term_ss = tok_ss
    mid_ss = (sq_ss, part_ss)
    turn(c_wgate, wgate_v, gatet_v)
    turn(c_wup, wup_v, upt_v)

    def spread(t, k):
        mix_f[t, pl.ds(k * RL, RL)] = mix_all[k, t].astype(F32).reshape(RL, H, DV)

    given = []
    for t in range(T):
        slot = mid_all.at[kv * T + t]
        for j in hops[::-1] + [0]:
            for peer in range(1 if j == 0 else T):
                given.append(
                    remote(slot, slot, mid_ss[t], mid_rs.at[kv, t], hop(j), peer)
                )

    @pl.when(tp == 1)
    def _():
        for j in [0] + hops:
            k = hop(j)
            if j:
                arrived(mix_all.at[k], mix_ss, mix_rs.at[k])
            for t in range(T):
                spread(t, k)
        every_head = jnp.concatenate(
            [mix_f[t, :, h, :].astype(BF16) for t in range(T) for h in range(H)], axis=1
        )
        pltpu.make_async_copy(w_out, wout_v.at[1], local_sem.at[3]).wait()
        arrived(wout_v.at[0], wout_ss, wout_rs)
        middle = [
            tok_v[t].astype(F32)
            + halves(every_head, wout_v.at[t])
            for t in range(T)
        ]
        for t in range(T):
            mid_all[kv * T + t] = middle[t].astype(BF16)
            for copy in given[t * len(given) // T : (t + 1) * len(given) // T]:
                copy.start()

    c_mlpg.wait()
    square = jnp.zeros((R, 1), F32)
    gate = None
    if W % 128 == 0:
        groups = [[(j, t)] for j in [0] + hops for t in range(T)]
    else:
        groups = [[(j, t) for t in range(T)] for j in [0] + hops]
    for group in groups:
        k = hop(group[0][0])
        for j, t in group:
            if j:
                arrived(mid_all.at[k * T + t], mid_ss[t], mid_rs.at[k, t])
            else:

                @pl.when(tp == 0)
                def _(t=t):
                    arrived(mid_all.at[kv * T + t], mid_ss[t], mid_rs.at[kv, t])

        j = k * T + group[0][1]
        blocks = []
        for i in range(len(group)):
            block = mid_all[j + i].astype(F32)
            square = square + jnp.sum(block * block, axis=1, keepdims=True)
            blocks.append((block * mlpg_v[j + i]).astype(BF16))
        block = jnp.concatenate(blocks, axis=1) if len(blocks) > 1 else blocks[0]
        width = len(group) * W
        lanes = pl.ds(pl.multiple_of(j * W, width), width)
        g = jnp.dot(block, gatet_v[lanes, :], preferred_element_type=F32)
        u = jnp.dot(block, upt_v[lanes, :], preferred_element_type=F32)
        gate, upward = (g, u) if gate is None else (gate + g, upward + u)
    mlp_scale = lax.rsqrt(square / D + epsilon)
    hidden = (silu(gate * mlp_scale) * (upward * mlp_scale)).astype(BF16)
    c_wdown.wait()
    span = 1 if W % 128 == 0 else T
    last = None

    def give(j, first, chunk):
        for t in range(first, first + span):
            slot = hop(j) * T + t
            term_send[slot] = chunk[:, (t - first) * W : (t - first + 1) * W].astype(BF16)
            copy = remote(term_send.at[slot], term_recv.at[me], term_ss, term_rs, hop(j), t)
            if j:
                copy.start()
            else:
                pl.when(tp != t)(copy.start)

    for j in hops[::-1] + [0]:
        for first in range(0, T, span):
            lanes = pl.ds(pl.multiple_of((hop(j) * T + first) * W, span * W), span * W)
            cut = hidden.shape[1] // 256 // 2 * 256
            chunk = jnp.dot(hidden[:, cut:], wdown_v[cut:, lanes], preferred_element_type=F32)
            if cut:
                chunk = chunk + jnp.dot(
                    hidden[:, :cut], wdown_v[:cut, lanes], preferred_element_type=F32
                )
            if last is not None:
                give(*last)
            last = (j, first, chunk)
    give(*last)
    value = summed(tp, 2, own_part(2))
    columns = forget.T
    for s in range(RL):
        for h in range(H):
            i = s * H + h
            row = value[i : i + 1, :]
            new_state[s, h] = row + columns[:, i : i + 1] * (past_v[s, h] - row)

    total = term_send[me].astype(F32)

    @pl.when(tp == 0)
    def _():
        left(part_send.at[pl.ds(0, 2), most], again_ss)
        for copy in pushes:
            copy.wait_send()

    @pl.when(tp == 1)
    def _():
        left(mix_all.at[most], mix_ss)
        for t in range(T):
            left(mid_all.at[pl.ds(0, K * T - 1)], mid_ss[t])

    arrived(term_recv.at[pl.ds(0, K * T - 1)], term_ss, term_rs)
    for dk, dt in near:
        k, t = source(dk, dt)
        total = total + term_recv[k * T + t].astype(F32)
    result[...] = (mid_all[me].astype(F32) + total).astype(BF16)
    left(term_send.at[pl.ds(0, K * T - 1)], term_ss)


def flush(result_v, state_v, result, new_state, sem):
    copies = [
        pltpu.make_async_copy(state_v, new_state, sem.at[0]),
        pltpu.make_async_copy(result_v, result, sem.at[1]),
    ]
    for copy in copies:
        copy.start()
    for copy in copies:
        copy.wait()


def body(
    tokens,
    past_state,
    mix_gain,
    w_query,
    w_forget,
    w_value,
    w_gate_out,
    floor_logits,
    head_gain,
    w_out,
    mlp_gain,
    w_gate,
    w_up,
    w_down,
):
    K = lax.axis_size("kv")
    T = lax.axis_size("tp")
    assert T == 2
    n = K * T
    R, W = tokens.shape
    RL, H, DK, DV = past_state.shape
    args = (
        tokens,
        past_state,
        mix_gain.reshape(T, 1, W),
        w_query,
        w_forget,
        w_value,
        w_gate_out,
        floor_logits.reshape(H, DK),
        head_gain.reshape(1, DV),
        w_out,
        mlp_gain.reshape(n, 1, W),
        w_gate.T,
        w_up.T,
        w_down,
    )
    V = pltpu.VMEM
    dma = pltpu.SemaphoreType.DMA
    anywhere = pl.BlockSpec(memory_space=pl.ANY)
    outs = pl.pallas_call(
        functools.partial(kernel, K, T),
        out_shape=(
            pltpu.VMEM((R, W), BF16),
            pltpu.VMEM(past_state.shape, F32),
        ),
        in_specs=[anywhere] * len(args),
        out_specs=(pl.BlockSpec(memory_space=pltpu.VMEM),)*2,
        scratch_shapes=[
            V((T, R, W), BF16),
            V(past_state.shape, F32),
            V((T, 1, W), F32),
            V((4,) + w_query.shape, BF16),
            V((T, H, DK), F32),
            V((1, DV), F32),
            V((T,) + w_out.shape, BF16),
            V((n, 1, W), F32),
            V(w_gate.shape[::-1], BF16),
            V(w_up.shape[::-1], BF16),
            V(w_gate.shape, BF16),
            V(w_up.shape, BF16),
            V(w_down.shape, BF16),
            V((K, RL, DK), F32),
            V((K, RL, DK), F32),
            V((4, R, H, DK), F32),
            V((4, K, RL * H, DK), BF16),
            V((T, 4, K, RL * H, DK), BF16),
            V((T, RL * H * DK, DV), BF16),
            V((K, T, RL * H, DV), BF16),
            V((T, R, H, DV), F32),
            V((n, R, W), BF16),
            V((n, R, W), BF16),
            V((n, R, W), BF16),
            dma((10,)),
            pltpu.SemaphoreType.REGULAR,
            dma,
            dma,
            dma,
            dma,
            dma,
            dma((T, 3)),
            dma,
            dma,
            dma,
            dma,
            dma,
            dma,
            dma,
            dma,
            dma((K,)),
            dma((K, T)),
            dma,
        ],
        compiler_params=pltpu.CompilerParams(
            collective_id=0, has_side_effects=True, vmem_limit_bytes=60 * 1024 * 1024
        ),
    )(*args)
    return pl.pallas_call(
        flush,
        out_shape=(
            jax.ShapeDtypeStruct((R, W), BF16),
            jax.ShapeDtypeStruct(past_state.shape, F32),
        ),
        in_specs=[pl.BlockSpec(memory_space=V)] * 2,
        out_specs=(anywhere,) * 2,
        scratch_shapes=[dma((2,))],
        compiler_params=pltpu.CompilerParams(vmem_limit_bytes=1024 * 1024),
    )(*outs)


def solution(mesh):
    placed = (
        P(("grp", "dp"), ("kv", "tp")),
        P(("grp", "dp", "kv"), "tp", None, None),
        P("kv"),
        P("kv", "tp"),
        P("kv", "tp"),
        P("kv", "tp"),
        P("kv", "tp"),
        P("tp"),
        P(),
        P(None, ("kv", "tp")),
        P(),
        P(None, ("kv", "tp")),
        P(None, ("kv", "tp")),
        P(("kv", "tp"), None),
    )
    return jax.shard_map(
        body,
        mesh=mesh,
        in_specs=placed,
        out_specs=(P(("grp", "dp"), ("kv", "tp")), P(("grp", "dp", "kv"), "tp", None, None)),
        check_vma=False,
    )
```

```python
import functools

import jax
import jax.numpy as jnp
from jax import lax
from jax.experimental import pallas as pl
from jax.experimental.pallas import tpu as pltpu
from jax.sharding import PartitionSpec as P

epsilon = 1e-06
F32 = jnp.float32
BF16 = jnp.bfloat16
MESH = pl.DeviceIdType.MESH


def sigmoid(a):
    return 1.0 / (1.0 + jnp.exp(-a))


def silu(a):
    return a / (1.0 + jnp.exp(-a))


def kernel(
    K,
    T,
    tokens,
    past,
    mix_gain,
    w_query,
    w_forget,
    w_value,
    w_gate_out,
    floor_logits,
    head_gain,
    w_out,
    mlp_gain,
    w_gate,
    w_up,
    w_down,
    result,
    new_state,
    tok_v,
    past_v,
    mixg_v,
    proj_v,
    floor_v,
    hgain_v,
    wout_v,
    mlpg_v,
    wgate_v,
    wup_v,
    gatet_v,
    upt_v,
    wdown_v,
    sq_send,
    sq_recv,
    part,
    part_send,
    part_recv,
    round_v,
    mix_all,
    mix_f,
    mid_all,
    term_send,
    term_recv,
    local_sem,
    ready,
    tok_ss,
    tok_rs,
    sq_ss,
    sq_rs,
    part_ss,
    part_rs,
    again_ss,
    floor_ss,
    floor_rs,
    past_ss,
    past_rs,
    wout_ss,
    wout_rs,
    mix_ss,
    mix_rs,
    mid_ss,
    mid_rs,
    term_ss,
    term_rs,
):
    R, W = tokens.shape
    RL, H, DK, DV = past.shape
    D = w_gate.shape[1]
    kv = lax.axis_index("kv")
    tp = lax.axis_index("tp")
    me = kv * T + tp

    hops = list(range(1, K))
    near = [(0, dt) for dt in range(1, T)] + [(j, dt) for j in hops for dt in range(T)]
    upper = (2 * kv) // K
    short = upper * (K - 1 - kv) + (1 - upper) * kv
    ahead = 1 - 2 * upper

    def hop(j):
        if j == 0:
            return kv
        both = jnp.minimum(jnp.maximum(2 * short - j + 1, 0), 1)
        step = both * ((j + 1) // 2) * (2 * (j % 2) - 1) + (1 - both) * (j - short)
        return kv + ahead * step

    def other(j, dt):
        return hop(j), (lax.rem(tp + dt, T) if j == 0 else dt)

    def source(j, dt):
        return hop(j), (lax.rem(tp + T - dt, T) if j == 0 else T - 1 - dt)

    def load(i, src, dst):
        copy = pltpu.make_async_copy(src, dst, local_sem.at[i])
        copy.start()
        return copy

    c_tok = load(0, tokens, tok_v.at[tp])
    c_mixg = load(1, mix_gain, mixg_v)
    c_proj = [
        load(2 + i, w, proj_v.at[i])
        for i, w in enumerate((w_forget, w_query, w_value, w_gate_out))
    ]
    c_past = load(6, past, past_v)
    c_floor = load(7, floor_logits, floor_v.at[tp])
    c_hgain = load(8, head_gain, hgain_v)
    c_mlpg = load(9, mlp_gain, mlpg_v)

    barrier = pltpu.get_barrier_semaphore()

    def signal(k, t):
        pl.semaphore_signal(barrier, inc=1, device_id={"kv": k, "tp": t}, device_id_type=MESH)

    for j in hops[::-1]:
        signal(hop(j), 0)

    @pl.when(tp == 0)
    def _():
        signal(kv, 1)

    @pl.when(tp == 1)
    def _():
        pl.semaphore_wait(barrier, 1)
        pl.semaphore_signal(ready, inc=1, device_id={"kv": kv, "tp": 0}, device_id_type=MESH)

    c_tok.wait()

    def remote(src, dst, ss, rs, k, t):
        return pltpu.make_async_remote_copy(
            src_ref=src,
            dst_ref=dst,
            send_sem=ss,
            recv_sem=rs,
            device_id={"kv": k, "tp": t},
            device_id_type=MESH,
        )

    def send(*args):
        copy = remote(*args)
        copy.start()
        return copy

    def arrived(dst, ss, rs):
        pltpu.make_async_remote_copy(
            src_ref=dst,
            dst_ref=dst,
            send_sem=ss,
            recv_sem=rs,
            device_id={"kv": kv, "tp": lax.rem(tp + 1, T)},
            device_id_type=MESH,
        ).wait_recv()

    def left(src, ss):
        pltpu.make_async_remote_copy(
            src_ref=src,
            dst_ref=src,
            send_sem=ss,
            recv_sem=tok_rs,
            device_id={"kv": kv, "tp": 1 - tp},
            device_id_type=MESH,
        ).wait_send()

    most = pl.ds(0, K - 1)
    swap = pltpu.make_async_remote_copy(
        src_ref=tok_v.at[tp],
        dst_ref=tok_v.at[tp],
        send_sem=tok_ss,
        recv_sem=tok_rs,
        device_id={"kv": kv, "tp": 1 - tp},
        device_id_type=MESH,
    )

    @pl.when(tp == 0)
    def _():
        pl.semaphore_wait(ready, 1)

    swap.start()
    c_mixg.wait()

    def features(t):
        block = tok_v[t].astype(F32)
        square = jnp.sum(block * block, axis=1, keepdims=True)
        rows = pl.ds(pl.multiple_of(t * W, W), W)
        return (block * mixg_v[t]).astype(BF16), rows, square

    def project(part_of, i):
        gained, rows, _ = part_of
        return jnp.dot(gained, proj_v[i, rows, :], preferred_element_type=F32)

    def spread_out(i, total):
        for h in range(H):
            part[i, :, h, :] = total[:, h * DK : (h + 1) * DK]
        for k in range(K):
            part_send[i, k] = part[i, k * RL : (k + 1) * RL].reshape(RL * H, DK).astype(BF16)

    def scatter(*which):
        for j in hops[::-1]:
            k = hop(j)
            for i in which:
                send(
                    part_send.at[i, k],
                    part_recv.at[tp, i, kv],
                    part_ss,
                    part_rs.at[tp, max(i - 1, 0)],
                    k,
                    1,
                )
        for i in which:
            own = remote(
                part_send.at[i, kv],
                part_recv.at[0, i, kv],
                part_ss,
                part_rs.at[0, max(i - 1, 0)],
                kv,
                1,
            )
            pl.when(tp == 0)(own.start)

    again = []
    mine = features(tp)
    early = []
    for i in range(2):
        c_proj[i].wait()
        early.append(project(mine, i))
    swap.wait_recv()
    theirs = features(1 - tp)
    square = jnp.broadcast_to(mine[2] + theirs[2], (R, DK))
    for k in range(K):
        sq_send[k] = square[k * RL : (k + 1) * RL]
    totals = [early[i] + project(theirs, i) for i in range(2)]
    spread_out(0, totals[0])
    spread_out(1, totals[1])

    @pl.when(tp == 0)
    def _():
        pl.semaphore_wait(barrier, (K - 1) * T)
        pl.semaphore_signal(ready, inc=1, device_id={"kv": kv, "tp": 1}, device_id_type=MESH)

    @pl.when(tp == 1)
    def _():
        pl.semaphore_wait(ready, 1)

    for j in hops[::-1]:
        k = hop(j)
        send(sq_send.at[k], sq_recv.at[kv], sq_ss, sq_rs, k, tp)
    scatter(0, 1)
    push = remote(w_out, wout_v.at[0], wout_ss, wout_rs, kv, 1)
    c_wgate = load(0, w_gate, wgate_v)
    c_wup = load(1, w_up, wup_v)
    c_wdown = load(2, w_down, wdown_v)
    totals = []
    for i in range(2, 4):
        c_proj[i].wait()
        totals.append(project(mine, i) + project(theirs, i))
    for i in range(2, 4):
        spread_out(i, totals[i - 2])
        scatter(i)

    for i in (0, 2):
        for j in hops[::-1]:
            k = hop(j)
            again.append(
                remote(
                    part_send.at[i, k],
                    part_recv.at[0, i, kv],
                    again_ss,
                    part_rs.at[0, max(i - 1, 0)],
                    k,
                    0,
                )
            )
    c_past.wait()
    for s in range(RL):
        for h in range(H):
            rows = pl.ds((s * H + h) * DK, DK)
            round_v[tp, rows, :] = past_v[s, h].astype(BF16)
    pushes = [
        remote(floor_logits, floor_v.at[0], floor_ss, floor_rs, kv, 1),
        remote(round_v.at[0], round_v.at[0], past_ss, past_rs, kv, 1),
        push,
    ]

    @pl.when(tp == 0)
    def _():
        for copy in pushes[:2] + again + pushes[2:]:
            copy.start()

    @pl.when(tp == 1)
    def _():
        pltpu.make_async_copy(w_out, wout_v.at[1], local_sem.at[3]).start()

    c_floor.wait()
    c_hgain.wait()
    square = sq_send[kv]
    arrived(sq_recv.at[most], sq_ss, sq_rs)
    for j in hops:
        square = square + sq_recv[hop(j)]
    row_scale = lax.rsqrt(square / D + epsilon)
    row_scale = jnp.concatenate(
        [jnp.broadcast_to(row_scale[s : s + 1], (H, DK)) for s in range(RL)], axis=0
    )

    def own_part(i):
        return part[i, pl.ds(kv * RL, RL)].reshape(RL * H, DK)

    def both(first, count):
        which = pl.ds(first, count)
        group = max(first - 1, 0)
        arrived(part_recv.at[0, which], part_ss, part_rs.at[0, group])
        arrived(part_recv.at[1, which, most], part_ss, part_rs.at[1, group])

    def summed(u, i, total):
        for j in hops:
            total = total + part_recv[u, i, hop(j)].astype(F32)
        return total * row_scale

    def total_of(u, i):
        own = part_recv[0, i, kv].astype(F32) if u == 0 else own_part(i)
        return summed(u, i, own)

    def forget_of(u, total):
        lower = sigmoid(floor_v[u])
        lower = jnp.concatenate([lower] * RL, axis=0)
        return lower + (1.0 - lower) * sigmoid(total)

    owner = lax.broadcasted_iota(jnp.int32, (RL * H, DK), 0)

    def weighted(u, forget, activ):
        weight = activ * forget
        left = jnp.concatenate(
            [jnp.where(owner == i, weight, 0.0).astype(BF16) for i in range(RL * H)], axis=1
        )
        return (
            halves(left, round_v.at[u]),
            jnp.sum(activ * (1.0 - forget), axis=1, keepdims=True),
        )

    def halves(a, b):
        cut = b.shape[0] // 2
        first = jnp.dot(a[:, :cut], b[:cut, :], preferred_element_type=F32)
        return first + jnp.dot(a[:, cut:], b[cut:, :], preferred_element_type=F32)

    def normed(head_out):
        return (
            head_out
            * lax.rsqrt(jnp.mean(head_out * head_out, axis=1, keepdims=True) + epsilon)
            * hgain_v[...]
        )

    @pl.when(tp == 0)
    def _():
        arrived(part_recv.at[0, 0, most], part_ss, part_rs.at[0, 0])
        arrived(part_recv.at[0, 2, most], part_ss, part_rs.at[0, 1])

    @pl.when(tp == 1)
    def _():
        both(0, 2)

    forget = forget_of(tp, summed(tp, 0, own_part(0)))
    mix_sends = [
        remote(mix_all.at[kv], mix_all.at[kv], mix_ss, mix_rs.at[kv], hop(j), 1)
        for j in hops[::-1]
    ]

    @pl.when(tp == 1)
    def _():
        arrived(floor_v.at[0], floor_ss, floor_rs)
        arrived(round_v.at[0], past_ss, past_rs)
        zero, zero_rest = weighted(0, forget_of(0, total_of(0, 0)), silu(total_of(0, 1)))
        one, one_rest = weighted(1, forget, silu(total_of(1, 1)))
        both(2, 1)
        zero = normed(zero + total_of(0, 2) * zero_rest)
        one = normed(one + total_of(1, 2) * one_rest)
        both(3, 1)
        mix_all[kv, 0] = (zero * silu(total_of(0, 3))).astype(BF16)
        mix_all[kv, 1] = (one * silu(total_of(1, 3))).astype(BF16)
        for copy in mix_sends:
            copy.start()

    def turn(copy, src, dst):
        copy.wait()
        step = 256 if D % 256 == 0 else D
        for c in range(0, D, step):
            dst[c : c + step, :] = src[:, c : c + step].T

    turn(c_wgate, wgate_v, gatet_v)
    c_wup.wait()

    def spread(t, k):
        mix_f[t, pl.ds(k * RL, RL)] = mix_all[k, t].astype(F32).reshape(RL, H, DV)

    given = []
    for t in range(T):
        slot = mid_all.at[kv * T + t]
        for j in hops[::-1] + [0]:
            for peer in range(1 if j == 0 else T):
                given.append(
                    remote(slot, slot, mid_ss.at[t], mid_rs.at[kv, t], hop(j), peer)
                )

    @pl.when(tp == 1)
    def _():
        for j in [0] + hops:
            k = hop(j)
            if j:
                arrived(mix_all.at[k], mix_ss, mix_rs.at[k])
            for t in range(T):
                spread(t, k)
        every_head = jnp.concatenate(
            [mix_f[t, :, h, :].astype(BF16) for t in range(T) for h in range(H)], axis=1
        )
        pltpu.make_async_copy(w_out, wout_v.at[1], local_sem.at[3]).wait()
        arrived(wout_v.at[0], wout_ss, wout_rs)
        middle = [
            tok_v[t].astype(F32)
            + halves(every_head, wout_v.at[t])
            for t in range(T)
        ]
        for t in range(T):
            mid_all[kv * T + t] = middle[t].astype(BF16)
            for copy in given[t * len(given) // T : (t + 1) * len(given) // T]:
                copy.start()

    c_mlpg.wait()
    square = jnp.zeros((R, 1), F32)
    gate = None
    if W % 128 == 0:
        groups = [[(j, t)] for j in [0] + hops for t in range(T)]
    else:
        groups = [[(j, t) for t in range(T)] for j in [0] + hops]
    for group in groups:
        k = hop(group[0][0])
        for j, t in group:
            if j:
                arrived(mid_all.at[k * T + t], mid_ss.at[t], mid_rs.at[k, t])
            else:

                @pl.when(tp == 0)
                def _(t=t):
                    arrived(mid_all.at[kv * T + t], mid_ss.at[t], mid_rs.at[kv, t])

        j = k * T + group[0][1]
        blocks = []
        for i in range(len(group)):
            block = mid_all[j + i].astype(F32)
            square = square + jnp.sum(block * block, axis=1, keepdims=True)
            blocks.append((block * mlpg_v[j + i]).astype(BF16))
        block = jnp.concatenate(blocks, axis=1) if len(blocks) > 1 else blocks[0]
        width = len(group) * W
        lanes = pl.ds(pl.multiple_of(j * W, width), width)
        g = jnp.dot(block, gatet_v[lanes, :], preferred_element_type=F32)
        u = lax.dot_general(block, wup_v[:, lanes], (((1,), (1,)), ((), ())), preferred_element_type=F32)
        gate, upward = (g, u) if gate is None else (gate + g, upward + u)
    mlp_scale = lax.rsqrt(square / D + epsilon)
    hidden = (silu(gate * mlp_scale) * (upward * mlp_scale)).astype(BF16)
    c_wdown.wait()
    span = 1 if W % 128 == 0 else T
    last = None

    def give(j, first, chunk):
        for t in range(first, first + span):
            slot = hop(j) * T + t
            term_send[slot] = chunk[:, (t - first) * W : (t - first + 1) * W].astype(BF16)
            copy = remote(term_send.at[slot], term_recv.at[me], term_ss, term_rs, hop(j), t)
            if j:
                copy.start()
            else:
                pl.when(tp != t)(copy.start)

    for j in hops[::-1] + [0]:
        for first in range(0, T, span):
            lanes = pl.ds(pl.multiple_of((hop(j) * T + first) * W, span * W), span * W)
            chunk = jnp.dot(hidden, wdown_v[:, lanes], preferred_element_type=F32)
            if last is not None:
                give(*last)
            last = (j, first, chunk)
    give(*last)
    value = summed(tp, 2, own_part(2))
    columns = forget.T
    for s in range(RL):
        for h in range(H):
            i = s * H + h
            row = value[i : i + 1, :]
            new_state[s, h] = row + columns[:, i : i + 1] * (past_v[s, h] - row)

    total = term_send[me].astype(F32)
    swap.wait_send()
    left(sq_send.at[most], sq_ss)

    @pl.when(tp == 0)
    def _():
        left(part_send, part_ss)
        left(part_send.at[pl.ds(0, 2), most], again_ss)
        for copy in pushes:
            copy.wait_send()

    @pl.when(tp == 1)
    def _():
        left(part_send.at[:, most], part_ss)
        left(mix_all.at[most], mix_ss)
        for t in range(T):
            left(mid_all.at[pl.ds(0, K * T - 1)], mid_ss.at[t])

    arrived(term_recv.at[pl.ds(0, K * T - 1)], term_ss, term_rs)
    for dk, dt in near:
        k, t = source(dk, dt)
        total = total + term_recv[k * T + t].astype(F32)
    result[...] = (mid_all[me].astype(F32) + total).astype(BF16)
    left(term_send.at[pl.ds(0, K * T - 1)], term_ss)


def flush(result_v, state_v, result, new_state, sem):
    copies = [
        pltpu.make_async_copy(state_v, new_state, sem.at[0]),
        pltpu.make_async_copy(result_v, result, sem.at[1]),
    ]
    for copy in copies:
        copy.start()
    for copy in copies:
        copy.wait()


def body(
    tokens,
    past_state,
    mix_gain,
    w_query,
    w_forget,
    w_value,
    w_gate_out,
    floor_logits,
    head_gain,
    w_out,
    mlp_gain,
    w_gate,
    w_up,
    w_down,
):
    K = lax.axis_size("kv")
    T = lax.axis_size("tp")
    assert T == 2
    n = K * T
    R, W = tokens.shape
    RL, H, DK, DV = past_state.shape
    args = (
        tokens,
        past_state,
        mix_gain.reshape(T, 1, W),
        w_query,
        w_forget,
        w_value,
        w_gate_out,
        floor_logits.reshape(H, DK),
        head_gain.reshape(1, DV),
        w_out,
        mlp_gain.reshape(n, 1, W),
        w_gate.T,
        w_up.T,
        w_down,
    )
    V = pltpu.VMEM
    dma = pltpu.SemaphoreType.DMA
    anywhere = pl.BlockSpec(memory_space=pl.ANY)
    outs = pl.pallas_call(
        functools.partial(kernel, K, T),
        out_shape=(
            pltpu.VMEM((R, W), BF16),
            pltpu.VMEM(past_state.shape, F32),
        ),
        in_specs=[anywhere] * len(args),
        out_specs=(pl.BlockSpec(memory_space=pltpu.VMEM),)*2,
        scratch_shapes=[
            V((T, R, W), BF16),
            V(past_state.shape, F32),
            V((T, 1, W), F32),
            V((4,) + w_query.shape, BF16),
            V((T, H, DK), F32),
            V((1, DV), F32),
            V((T,) + w_out.shape, BF16),
            V((n, 1, W), F32),
            V(w_gate.shape[::-1], BF16),
            V(w_up.shape[::-1], BF16),
            V(w_gate.shape, BF16),
            V(w_up.shape, BF16),
            V(w_down.shape, BF16),
            V((K, RL, DK), F32),
            V((K, RL, DK), F32),
            V((4, R, H, DK), F32),
            V((4, K, RL * H, DK), BF16),
            V((T, 4, K, RL * H, DK), BF16),
            V((T, RL * H * DK, DV), BF16),
            V((K, T, RL * H, DV), BF16),
            V((T, R, H, DV), F32),
            V((n, R, W), BF16),
            V((n, R, W), BF16),
            V((n, R, W), BF16),
            dma((10,)),
            pltpu.SemaphoreType.REGULAR,
            dma,
            dma,
            dma,
            dma,
            dma,
            dma((T, 3)),
            dma,
            dma,
            dma,
            dma,
            dma,
            dma,
            dma,
            dma,
            dma((K,)),
            dma((T,)),
            dma((K, T)),
            dma,
            dma,
        ],
        compiler_params=pltpu.CompilerParams(
            collective_id=0, has_side_effects=True, vmem_limit_bytes=60 * 1024 * 1024
        ),
    )(*args)
    return pl.pallas_call(
        flush,
        out_shape=(
            jax.ShapeDtypeStruct((R, W), BF16),
            jax.ShapeDtypeStruct(past_state.shape, F32),
        ),
        in_specs=[pl.BlockSpec(memory_space=V)] * 2,
        out_specs=(anywhere,) * 2,
        scratch_shapes=[dma((2,))],
        compiler_params=pltpu.CompilerParams(vmem_limit_bytes=1024 * 1024),
    )(*outs)


def solution(mesh):
    placed = (
        P(("grp", "dp"), ("kv", "tp")),
        P(("grp", "dp", "kv"), "tp", None, None),
        P("kv"),
        P("kv", "tp"),
        P("kv", "tp"),
        P("kv", "tp"),
        P("kv", "tp"),
        P("tp"),
        P(),
        P(None, ("kv", "tp")),
        P(),
        P(None, ("kv", "tp")),
        P(None, ("kv", "tp")),
        P(("kv", "tp"), None),
    )
    return jax.shard_map(
        body,
        mesh=mesh,
        in_specs=placed,
        out_specs=(P(("grp", "dp"), ("kv", "tp")), P(("grp", "dp", "kv"), "tp", None, None)),
        check_vma=False,
    )
```
